512 devices in a mesh: kv: 64 (over z, y), tp: 8 (over x, core).
Axes of the slice: x: 4, y: 4, z: 16, core: 2. Of those that a mesh axis runs over, the one named last changes fastest.
Arguments:
- tokens: bfloat16 [256, 4096], P(None, 'kv')
- lengths: int32 [64], replicated, may hold values from 1 to 4, 112 in all
- memory: float32 [64, 16, 128, 128], P('kv', 'tp'), may hold values from -0.6 to 0.6
- norm_gain: float32 [4096], P('kv'), may hold values from 0.1 to 1.9
- w_query: bfloat16 [4096, 2048], P('kv', 'tp'), may hold values from -0.09375 to 0.09375
- w_key: bfloat16 [4096, 2048], P('kv', 'tp'), may hold values from -0.09375 to 0.09375
- w_value: bfloat16 [4096, 2048], P('kv', 'tp'), may hold values from -0.09375 to 0.09375
- w_outgate: bfloat16 [4096, 2048], P('kv', 'tp'), may hold values from -0.09375 to 0.09375
- w_alpha: bfloat16 [4096, 16], P('kv'), may hold values from -0.09375 to 0.09375
- w_beta: bfloat16 [4096, 16], P('kv'), may hold values from -0.09375 to 0.09375
- decay_log: float32 [16], P('tp'), may hold values from -4 to 0.5
- decay_bias: float32 [16], P('tp'), may hold values from -1 to 1
- head_gain: float32 [128], replicated, may hold values from 0.1 to 1.9
- w_output: bfloat16 [2048, 4096], P('tp', 'kv'), may hold values from -0.125 to 0.125
- mlp_gain: float32 [4096], P('kv'), may hold values from 0.1 to 1.9
- w_gate: bfloat16 [4096, 11264], P('kv', 'tp'), may hold values from -0.09375 to 0.09375
- w_up: bfloat16 [4096, 11264], P('kv', 'tp'), may hold values from -0.09375 to 0.09375
- w_down: bfloat16 [11264, 4096], P('tp', 'kv'), may hold values from -0.0546875 to 0.0546875
Outputs:
- layer_out: bfloat16 [256, 4096], P(None, 'kv')
- new_memory: float32 [64, 16, 128, 128], P('kv', 'tp')
The draws below stay inside these ranges and needn't reach their ends.
Inputs may be any that keep to these rules, and one draw needn't show every extreme that they name: How many of a sequence's 4 slots hold live tokens; the live ones come first; the lengths add up to seven quarters of 64, rounded down.
All inputs are finite; a program needn't handle non-finite values.
Results may differ from the reference program's by a relative error of at most 0.012.
Values may be sent and summed in bfloat16 or wider, within the bound.
A program may use at most 64 MiB of HBM per device.

```python
import math
import jax
import jax.numpy as jnp
import numpy as np
from jax import lax

D = 4096
H = 16
DK = 128
DV = 128
FF = 11264
NEW = 4
SEQS = 64


def draw_tokens(key, part):
    first, second, third = jax.random.split(key, 3)
    total_rows = SEQS * NEW
    column_ramp = jnp.exp(jnp.linspace(math.log(0.5), math.log(2.0), D))
    column_noise = jnp.exp(jax.random.uniform(second, (D,), jnp.float32, math.log(0.7), math.log(1.4)))
    row_scale = jnp.exp(jax.random.uniform(third, (total_rows, 1), jnp.float32, math.log(0.3), math.log(3.0)))
    base = jax.random.normal(first, (total_rows, D), jnp.float32)
    return (base * column_ramp * column_noise * row_scale).astype(jnp.bfloat16)


def level_of(key, extent, pieces, least, largest):
    level = 1.0
    for position, parts in pieces:
        draws = jax.random.uniform(jax.random.fold_in(jax.random.fold_in(key, 6), position), (parts,), jnp.float32, least / len(pieces), largest / len(pieces))
        level = level * jnp.repeat(jnp.exp(draws), extent[position] // parts).reshape((-1,) + (1,) * (len(extent) - 1 - position))
    return level


def length_profile(count, total, reach, slope):
    weights = [(1 << 20) // math.isqrt(rank ** slope) + 1 for rank in range(2, count + 1)]
    surplus, counts = total - reach - (count - 1), [1] * (count - 1)
    while surplus > 0:
        movable = [i for i in range(count - 1) if counts[i] < reach]
        whole, budget = sum([weights[i] for i in movable]), surplus
        for i in movable:
            more = min(reach - counts[i], max(1, budget * weights[i] // whole), surplus)
            counts[i] = counts[i] + more
            surplus = surplus - more
    return np.array([reach] + counts)


def ragged(stream_key, count, total, bound, slope):
    if count == 2:
        one = jax.random.randint(stream_key, (), max(1, total - bound), min(bound, total - 1) + 1)
        return jnp.stack([one, total - one])
    sizes = jnp.asarray(length_profile(count, total, bound, slope), jnp.int32)
    pairs = (count - 1) // 2
    giver, sink = sizes[1:1 + 2 * pairs:2], sizes[2:2 + 2 * pairs:2]
    room = jnp.minimum(giver - 1, bound - sink)
    passed = jax.random.randint(jax.random.fold_in(stream_key, 1), (pairs,), 0, 1 << 20) % (room + 1)
    sizes = sizes.at[1:1 + 2 * pairs:2].set(giver - passed).at[2:2 + 2 * pairs:2].set(sink + passed)
    return sizes[jax.random.permutation(jax.random.fold_in(stream_key, 2), count)]


def centred(rng, extent, spread, bound, cuts=(), held_as=jnp.bfloat16):
    gain = level_of(rng, extent, cuts, -0.22, 0.18) if cuts else 1.0
    values = jax.random.normal(rng, extent, jnp.float32) * spread * gain
    return jnp.minimum(jnp.maximum(values, -bound), bound).astype(held_as)


def setup_inputs(seed: int = 0) -> dict:
    streams_of = jax.random.split(jax.random.key(seed), 19)
    return {
        "tokens": draw_tokens(jax.random.fold_in(streams_of[18], 71), 0),
        "lengths": ragged(streams_of[1], SEQS, SEQS * 7 // 4, NEW, 2).astype(jnp.int32),
        "memory": centred(streams_of[2], (SEQS, H, DK, DV), 0.1, 0.6, ((0, 64), (1, 8)), jnp.float32),
        "norm_gain": jnp.clip(1.0 + 0.18 * jax.random.normal(streams_of[3], (D,), jnp.float32), 0.1, 1.9),
        "w_query": centred(streams_of[4], (D, H * DK), D ** -0.5, 0.09375, ((0, 64), (1, 8))),
        "w_key": centred(streams_of[5], (D, H * DK), D ** -0.5, 0.09375, ((0, 64), (1, 8))),
        "w_value": centred(streams_of[6], (D, H * DV), D ** -0.5, 0.09375, ((0, 64), (1, 8))),
        "w_outgate": centred(streams_of[7], (D, H * DV), D ** -0.5, 0.09375, ((0, 64), (1, 8))),
        "w_alpha": centred(streams_of[8], (D, H), D ** -0.5, 0.09375, ((0, 64),)),
        "w_beta": centred(streams_of[9], (D, H), D ** -0.5, 0.09375, ((0, 64),)),
        "decay_log": jnp.clip(-4.0 + 4.5 * jax.random.uniform(streams_of[10], (H,), jnp.float32) ** level_of(streams_of[10], (H,), ((0, 8),), -0.2, 0.2), -4.0, 0.5),
        "decay_bias": jnp.clip(jax.random.uniform(streams_of[11], (H,), jnp.float32, -1.0, 1.0) * level_of(streams_of[11], (H,), ((0, 8),), -0.4, 0.0), -1.0, 1.0),
        "head_gain": jnp.clip(1.0 + 0.18 * jax.random.normal(streams_of[12], (DV,), jnp.float32), 0.1, 1.9),
        "w_output": centred(streams_of[13], (H * DV, D), (H * DV) ** -0.5, 0.125, ((0, 8), (1, 64))),
        "mlp_gain": jnp.clip(1.0 + 0.18 * jax.random.normal(streams_of[14], (D,), jnp.float32), 0.1, 1.9),
        "w_gate": centred(streams_of[15], (D, FF), D ** -0.5, 0.09375, ((0, 64), (1, 8))),
        "w_up": centred(streams_of[16], (D, FF), D ** -0.5, 0.09375, ((0, 64), (1, 8))),
        "w_down": centred(streams_of[17], (FF, D), FF ** -0.5, 0.0546875, ((0, 8), (1, 64))),
    }


epsilon = 1e-06

def unit_rows(values):
    return values * lax.rsqrt(lax.optimization_barrier(jnp.sum(values * values, axis=-1, keepdims=True)) + epsilon)

def advance(memory, queries, key_rows, value_rows, decays, betas):
    outputs = []
    for step in range(queries.shape[1]):
        memory = jnp.exp(decays[:, step])[:, :, None, None] * memory
        predicted = jnp.einsum('shde,shd->she', memory, key_rows[:, step], precision=lax.Precision.HIGHEST)
        correction = betas[:, step][:, :, None] * (value_rows[:, step] - predicted)
        memory = memory + key_rows[:, step][:, :, :, None] * correction[:, :, None, :]
        outputs.append(jnp.einsum('shde,shd->she', memory, queries[:, step], precision=lax.Precision.HIGHEST))
    return (memory, jnp.stack(outputs, axis=1))

def reference(tokens, lengths, memory, norm_gain, w_query, w_key, w_value, w_outgate, w_alpha, w_beta, decay_log, decay_bias, head_gain, w_output, mlp_gain, w_gate, w_up, w_down):
    total_rows = tokens.shape[0]
    token_f = tokens.astype(jnp.float32)
    rstd = lax.rsqrt(lax.optimization_barrier(jnp.mean(token_f * token_f, axis=1, keepdims=True)) + epsilon)
    scaled = (token_f * norm_gain).astype(jnp.bfloat16)

    def project(weight):
        return jnp.dot(scaled, weight, preferred_element_type=jnp.float32) * rstd
    queries = project(w_query).astype(jnp.bfloat16)
    key_rows = project(w_key).astype(jnp.bfloat16)
    value_rows = project(w_value).astype(jnp.bfloat16)
    outgate = project(w_outgate).astype(jnp.bfloat16)
    alphas = project(w_alpha)
    beta_pre = project(w_beta)
    live = jnp.arange(NEW, dtype=jnp.int32)[None, :] < lengths[:, None]
    query_h = unit_rows(queries.astype(jnp.float32).reshape(SEQS, NEW, H, DK)) * DK ** (-0.5)
    key_h = unit_rows(key_rows.astype(jnp.float32).reshape(SEQS, NEW, H, DK))
    value_h = value_rows.astype(jnp.float32).reshape(SEQS, NEW, H, DV)
    decays = -jnp.exp(decay_log) * jax.nn.softplus(alphas + decay_bias)
    decays = jnp.where(live[:, :, None], decays.reshape(SEQS, NEW, H), 0.0)
    betas = jnp.where(live[:, :, None], jax.nn.sigmoid(beta_pre).reshape(SEQS, NEW, H), 0.0)
    new_memory, attended = advance(memory, query_h, key_h, value_h, decays, betas)
    attended = attended * lax.rsqrt(lax.optimization_barrier(jnp.mean(attended * attended, axis=-1, keepdims=True)) + epsilon)
    gate_h = outgate.astype(jnp.float32).reshape(SEQS, NEW, H, DV)
    mixed = (attended * head_gain * jax.nn.silu(gate_h)).astype(jnp.bfloat16).reshape(total_rows, H * DV)
    hidden = (token_f + jnp.dot(mixed, w_output, preferred_element_type=jnp.float32)).astype(jnp.bfloat16)
    hidden_f = hidden.astype(jnp.float32)
    rstd2 = lax.rsqrt(lax.optimization_barrier(jnp.mean(hidden_f * hidden_f, axis=1, keepdims=True)) + epsilon)
    hscaled = (hidden_f * mlp_gain).astype(jnp.bfloat16)
    gate_rows = jnp.dot(hscaled, w_gate, preferred_element_type=jnp.float32) * rstd2
    up_rows = jnp.dot(hscaled, w_up, preferred_element_type=jnp.float32) * rstd2
    active = (jax.nn.silu(gate_rows) * up_rows).astype(jnp.bfloat16)
    result = hidden_f + jnp.dot(active, w_down, preferred_element_type=jnp.float32)
    layer_out = jnp.where(live.reshape(total_rows)[:, None], result, 0.0).astype(jnp.bfloat16)
    return (layer_out, new_memory)
```

```python
import jax
import jax.numpy as jnp
from jax import lax
from jax.experimental import pallas as pl
from jax.experimental.pallas import tpu as pltpu
from jax.sharding import PartitionSpec as P

MESH = pl.DeviceIdType.MESH
F32, BF16, I32 = jnp.float32, jnp.bfloat16, jnp.int32
D, DK, NEW, SEQS = 4096, 128, 4, 64
Z, Y, TP = 16, 4, 8
ROWS = SEQS * NEW
PLACES = 8 * Z
EPS = 1e-06
W1 = 640
FFY = 352
FP = 384
W2 = 2 * FP
PH = 13
S_Y, S_Z, S_M, S_C, S_H, S_G, S_A, S_F, S_O, S_WO, S_WG, S_WD, S_GN = range(PH)


def iota(shape, dim):
    return lax.broadcasted_iota(I32, shape, dim)


def mm(a, b):
    return jnp.dot(a, b, preferred_element_type=F32)


def kernel(
    tok_ref, lens_ref, lencol_ref, mem_ref, ngain_ref, wq_ref, wk_ref, wv_ref, wg_ref, wa_ref, wb_ref,
    dlog_ref, dbias_ref, hgain_ref, wout_ref, mgain_ref, wgate_ref, wup_ref, wdown_ref,
    out_ref, nmem_ref,
    part, yrecv, zs1, zr1, mrecv, cs, cr, hbuf, wgs, wgr, wob, wdb, gl, gb, zs2, zr2, ab, fs, fr, ob, hct, wab,
    send, recv,
):
    kv = lax.axis_index("kv")
    tp = lax.axis_index("tp")
    z = kv // Y
    y = kv % Y
    group = y * TP + tp

    def y_peer(k):
        return z * Y + (y + k) % Y

    def z_peer(j):
        away = 8 - (j + 1) // 2
        return (z + Z + away * (2 * (j % 2) - 1)) % Z

    barrier = pltpu.get_barrier_semaphore()

    def greet_group(j, c):
        other = (group + j) % (Y * TP)
        pl.semaphore_signal(barrier, inc=1, device_id=(z * Y + other // TP, other % TP), device_id_type=MESH)
        return c

    def greet_z(j, c):
        pl.semaphore_signal(barrier, inc=1, device_id=(z_peer(j) * Y + y, tp), device_id_type=MESH)
        return c

    lax.fori_loop(0, Z - 1, greet_z, 0)
    lax.fori_loop(1, Y * TP, greet_group, 0)

    def rcopy(src, dst, phase, where):
        return pltpu.make_async_remote_copy(
            src_ref=src, dst_ref=dst, send_sem=send.at[phase], recv_sem=recv.at[phase],
            device_id=where, device_id_type=MESH,
        )

    def arrived(ref, phase):
        rcopy(ref, ref, phase, (y_peer(1), tp)).wait_recv()

    def sent(ref, phase):
        rcopy(ref, ref, phase, (y_peer(1), tp)).wait_send()

    tok_f = tok_ref[...].astype(F32)
    tok_b = tok_ref[...]
    scaled = (tok_f * ngain_ref[...]).astype(BF16)
    at = iota((2 * ROWS, ROWS), 0)
    row = iota((2 * ROWS, ROWS), 1)
    wanted = 16 * ((at >> 3) & 15) + 4 * (at >> 7) + (at & 3)
    turn = jnp.where(row == wanted, 1.0, 0.0).astype(BF16)
    xs = mm(turn, scaled).astype(BF16)
    xt = mm(turn, tok_b)
    wab[...] = jnp.zeros((64, 128), BF16)
    wab[:, 64:80] = wa_ref[...]
    wab[:, 80:96] = wb_ref[...]
    squares = jnp.sum(xt * xt, axis=1, keepdims=True)
    high = squares.astype(BF16).astype(F32)
    low = squares - high
    eye = jnp.where(iota((64, 128), 0) == iota((64, 128), 1), 1.0, 0.0).astype(BF16)
    lane = iota((2 * ROWS, 128), 1)
    extra = mm(xs, wab[...]) + mm(xt.astype(BF16), eye)
    extra = jnp.where(lane == 96, high, jnp.where(lane == 97, low, extra))
    second = (iota((2 * ROWS, 256), 0) & 4) == 4
    left = jnp.where(second, mm(xs, wv_ref[...]), mm(xs, wq_ref[...]))
    part[:, :, :, 0:256] = left.reshape(Y, Z, 8, 256).astype(BF16)
    right = jnp.where(second, mm(xs, wg_ref[...]), mm(xs, wk_ref[...]))
    part[:, :, :, 256:512] = right.reshape(Y, Z, 8, 256).astype(BF16)
    part[:, :, :, 512:640] = extra.reshape(Y, Z, 8, 128).astype(BF16)

    for k in range(Y):
        wgs[k, :, 0:FFY] = wgate_ref[:, FFY * k : FFY * (k + 1)]
        wgs[k, :, FFY:FP] = jnp.zeros((64, FP - FFY), BF16)
        wgs[k, :, FP : FP + FFY] = wup_ref[:, FFY * k : FFY * (k + 1)]
        wgs[k, :, FP + FFY : W2] = jnp.zeros((64, FP - FFY), BF16)
        wdb[k, FFY:FP, :] = jnp.zeros((FP - FFY, 64), BF16)
    gl[...] = jnp.zeros((8, 128), F32) + jnp.concatenate([mgain_ref[...], mgain_ref[...]], axis=1)

    pl.semaphore_wait(barrier, Z - 1 + Y * TP - 1)

    for k in range(1, Y):
        peer = y_peer(k)
        rcopy(part.at[peer % Y], yrecv.at[y], S_Y, (peer, tp)).start()
    for k in range(1, Y):
        peer = y_peer(k)
        rcopy(wout_ref, wob.at[y], S_WO, (peer, tp)).start()
        rcopy(wgs.at[peer % Y], wgr.at[y], S_WG, (peer, tp)).start()
        rcopy(
            wdown_ref.at[pl.ds(pl.multiple_of((peer % Y) * FFY, 16), FFY)], wdb.at[y, pl.ds(0, FFY)], S_WD, (peer, tp)
        ).start()
        rcopy(gl, gb.at[y], S_GN, (peer, tp)).start()

    yrecv[y] = part[y]
    wob[y] = wout_ref[...]
    wgr[y] = wgs[y]
    wdb[y, 0:FFY, :] = wdown_ref[pl.ds(pl.multiple_of(y * FFY, 16), FFY), :]
    gb[y] = gl[...]

    seq = iota((SEQS, ROWS), 0)
    lens = lencol_ref[...] + jnp.zeros((SEQS, ROWS), I32)
    place = iota((PLACES, ROWS), 0)

    def chooser(seq_of, slot):
        mine = jnp.sum(jnp.where(seq == seq_of, lens, 0), axis=0, keepdims=True)
        before = jnp.sum(jnp.where(seq < seq_of, lens, 0), axis=0, keepdims=True)
        slot = slot[0:1]
        index = before + slot
        chunk = (index * 9363) >> 16
        goes = jnp.where(slot < mine, index + chunk, -1)
        return jnp.where(place == goes, 1.0, 0.0).astype(BF16)

    col = iota((SEQS, ROWS), 1)
    pick = chooser(4 * ((col >> 2) & 15) + (col >> 6), col & 3)
    give = chooser(col >> 2, col & 3)

    arrived(yrecv.at[0:3], S_Y)
    total = yrecv[0].astype(F32)
    for k in range(1, Y):
        total = total + yrecv[k].astype(F32)
    zs1[...] = total.astype(BF16)

    def send_z1(j, c):
        to = z_peer(j)
        rcopy(zs1.at[to], zr1.at[z], S_Z, (to * Y + y, tp)).start()
        return c

    lax.fori_loop(0, Z - 1, send_z1, 0)
    zr1[z] = zs1[z]
    arrived(zr1.at[0 : Z - 1], S_Z)

    mine = jnp.sum(zr1[...].astype(F32), axis=0)
    lane8 = iota((8, 128), 1)
    ext = mine[:, 512:640]

    def lane_of(values, where):
        return jnp.sum(jnp.where(lane8 == where, values, 0.0), axis=1, keepdims=True)

    rstd = lax.rsqrt((lane_of(ext, 96) + lane_of(ext, 97)) / D + EPS)
    main = (mine[:, 0:512] * rstd).astype(BF16).astype(F32)
    ext = ext * rstd
    live = iota((8, 1), 0) < lens_ref[kv]
    rows = []
    for h in range(2):
        alpha = lane_of(ext, 64 + 2 * tp + h)
        beta = jax.nn.sigmoid(lane_of(ext, 80 + 2 * tp + h))
        shifted = alpha + dbias_ref[0, h]
        soft = jnp.maximum(shifted, 0.0) + jnp.log1p(jnp.exp(-jnp.abs(shifted)))
        rate = jnp.exp(jnp.zeros((8, 1), F32) + dlog_ref[0, h])
        decay = jnp.exp(jnp.where(live, -rate * soft, 0.0))
        beta = jnp.where(live, beta, 0.0)
        q8 = main[:, 128 * h : 128 * h + 128]
        k8 = main[:, 256 + 128 * h : 384 + 128 * h]
        q8 = q8 * lax.rsqrt(jnp.sum(q8 * q8, axis=1, keepdims=True) + EPS) * DK**-0.5
        k8 = k8 * lax.rsqrt(jnp.sum(k8 * k8, axis=1, keepdims=True) + EPS)
        qt, kt = q8.T, k8.T
        memory = mem_ref[0, h]
        for t in range(NEW):
            kcol = kt[:, t : t + 1]
            memory = memory * decay[t : t + 1]
            guess = jnp.sum(memory * kcol, axis=0, keepdims=True)
            fix = beta[t : t + 1] * (main[4 + t : 5 + t, 128 * h : 128 * h + 128] - guess)
            memory = memory + kcol * fix
            rows.append(jnp.sum(memory * qt[:, t : t + 1], axis=0, keepdims=True))
        nmem_ref[0, h] = memory
    attended = jnp.concatenate(rows, axis=0)
    attended = attended * lax.rsqrt(jnp.mean(attended * attended, axis=1, keepdims=True) + EPS)
    gates = jnp.concatenate([main[4:8, 256:384], main[4:8, 384:512]], axis=0)
    mixed = attended * hgain_ref[...] * (gates * jax.nn.sigmoid(gates))
    mrecv[z] = mixed.astype(BF16)

    def send_m(j, c):
        rcopy(mrecv.at[z], mrecv.at[z], S_M, (z_peer(j) * Y + y, tp)).start()
        return c

    lax.fori_loop(0, Z - 1, send_m, 0)
    arrived(wob.at[0:3], S_WO)
    wo = jnp.concatenate([wob[k].astype(F32) for k in range(Y)], axis=1).astype(BF16)
    arrived(gb.at[0:3], S_GN)
    low_lane = iota((1, 128), 1) < 64
    gain = jnp.concatenate(
        [jnp.where(low_lane, gb[0, 0:1], gb[1, 0:1]), jnp.where(low_lane, gb[2, 0:1], gb[3, 0:1])], axis=1
    )
    low_half = iota((8, 128), 0) < 4

    def kept(k):
        return jnp.where(
            low_half, yrecv[k, 2 * tp, :, 512:640].astype(F32), yrecv[k, 2 * tp + 1, :, 512:640].astype(F32)
        )

    residual = jnp.concatenate(
        [
            jnp.where(low_lane, kept(0), pltpu.roll(kept(1), 64, 1)),
            jnp.where(low_lane, kept(2), pltpu.roll(kept(3), 64, 1)),
        ],
        axis=1,
    )
    arrived(mrecv.at[0 : Z - 1], S_M)

    heads = mrecv[...].astype(F32).reshape(8 * Z, 128).astype(BF16)
    first_head = (iota((8 * Z, 256), 0) & 4) == 0
    terms = jnp.where(first_head, mm(heads, wo[0:128]), mm(heads, wo[128:256]))
    terms = terms.reshape(TP, 2, 8, 256)
    even, odd = terms[:, 0], terms[:, 1]
    even = even + jnp.concatenate([even[:, 4:8], even[:, 0:4]], axis=1)
    odd = odd + jnp.concatenate([odd[:, 4:8], odd[:, 0:4]], axis=1)
    cs[...] = jnp.where((iota((TP, 8, 256), 1) & 4) == 0, even, odd)

    def send_c(j, c):
        to = (tp + j) % TP
        rcopy(cs.at[to], cr.at[tp], S_C, (kv, to)).start()
        return c

    lax.fori_loop(1, TP, send_c, 0)
    cr[tp] = cs[tp]
    arrived(cr.at[0 : TP - 1], S_C)
    hbuf[group] = (residual + jnp.sum(cr[...], axis=0)).astype(BF16)

    def send_h(j, c):
        other = (group + j) % (Y * TP)
        rcopy(hbuf.at[group], hbuf.at[group], S_H, (z * Y + other // TP, other % TP)).start()
        return c

    lax.fori_loop(1, Y * TP, send_h, 0)
    arrived(wgr.at[0:3], S_WG)
    arrived(hbuf.at[0 : Y * TP - 1], S_H)

    hidden = mm(pick, hbuf[...].astype(F32).reshape(ROWS, 256).astype(BF16))
    hscaled = (hidden * gain).astype(BF16)
    products = mm(hscaled, wgr[...].reshape(256, W2))
    squares2 = jnp.sum(hidden * hidden, axis=1, keepdims=True)
    high2 = squares2.astype(BF16).astype(F32)
    low2 = squares2 - high2
    lane2 = iota((PLACES, W2), 1)
    products = jnp.where(lane2 == FFY, high2, jnp.where(lane2 == FFY + 1, low2, products))
    zs2[...] = products.reshape(Z, 8, W2).astype(BF16)

    def send_g(j, c):
        to = z_peer(j)
        rcopy(zs2.at[to], zr2.at[z], S_G, (to * Y + y, tp)).start()
        return c

    lax.fori_loop(0, Z - 1, send_g, 0)
    zr2[z] = zs2[z]
    hct[...] = hidden.T
    arrived(wdb.at[0:3, 0:FFY], S_WD)
    arrived(zr2.at[0 : Z - 1], S_G)
    summed = jnp.sum(zr2[...].astype(F32), axis=0)
    lane3 = iota((8, FP), 1)
    gate, up = summed[:, 0:FP], summed[:, FP:W2]
    total2 = jnp.sum(jnp.where((lane3 == FFY) | (lane3 == FFY + 1), gate, 0.0), axis=1, keepdims=True)
    rstd2 = lax.rsqrt(total2 / D + EPS)
    gate = jnp.where(lane3 < FFY, gate, 0.0) * rstd2
    ab[z] = (gate * jax.nn.sigmoid(gate) * (up * rstd2)).astype(BF16)

    def send_a(j, c):
        rcopy(ab.at[z], ab.at[z], S_A, (z_peer(j) * Y + y, tp)).start()
        return c

    lax.fori_loop(0, Z - 1, send_a, 0)
    arrived(ab.at[0 : Z - 1], S_A)

    active = ab[...].astype(F32).reshape(PLACES, FP).astype(BF16)
    for k in range(Y):
        fed = lax.dot_general(wdb[k], active, (((0,), (1,)), ((), ())), preferred_element_type=F32)
        fs[TP * k : TP * (k + 1)] = fed.reshape(TP, 8, 128)

    def send_f(j, c):
        other = (group + j) % (Y * TP)
        rcopy(fs.at[other], fr.at[group], S_F, (z * Y + other // TP, other % TP)).start()
        return c

    lax.fori_loop(1, Y * TP, send_f, 0)
    fr[group] = fs[group]
    arrived(fr.at[0 : Y * TP - 1], S_F)
    ended = jnp.sum(fr[...], axis=0) + hct[pl.ds(pl.multiple_of(8 * group, 8), 8), :]
    ob[tp] = ended.astype(BF16)

    def send_o(j, c):
        rcopy(ob.at[tp], ob.at[tp], S_O, (kv, (tp + j) % TP)).start()
        return c

    lax.fori_loop(1, TP, send_o, 0)
    arrived(ob.at[0 : TP - 1], S_O)
    final = ob[...].astype(F32).reshape(64, PLACES).astype(BF16)
    out_ref[...] = lax.dot_general(give, final, (((0,), (1,)), ((), ())), preferred_element_type=F32).astype(BF16)

    for ref, phase in (
        (yrecv.at[0:3], S_Y), (zr1.at[0 : Z - 1], S_Z), (mrecv.at[0 : Z - 1], S_M), (cr.at[0 : TP - 1], S_C),
        (hbuf.at[0 : Y * TP - 1], S_H), (zr2.at[0 : Z - 1], S_G), (ab.at[0 : Z - 1], S_A),
        (fr.at[0 : Y * TP - 1], S_F), (ob.at[0 : TP - 1], S_O), (wob.at[0:3], S_WO), (wgr.at[0:3], S_WG),
        (wdb.at[0:3, 0:FFY], S_WD), (gb.at[0:3], S_GN),
    ):
        sent(ref, phase)


def per_device(
    tokens, lengths, memory, norm_gain, w_query, w_key, w_value, w_outgate, w_alpha, w_beta, decay_log, decay_bias,
    head_gain, w_output, mlp_gain, w_gate, w_up, w_down,
):
    vmem = pl.BlockSpec(memory_space=pltpu.VMEM)
    smem = pl.BlockSpec(memory_space=pltpu.SMEM)
    return tuple(
        pl.pallas_call(
            kernel,
            out_shape=(
                jax.ShapeDtypeStruct(tokens.shape, BF16),
                jax.ShapeDtypeStruct(memory.shape, F32),
            ),
            in_specs=[vmem, smem] + [vmem] * 9 + [smem, smem] + [vmem] * 6,
            out_specs=(vmem, vmem),
            scratch_shapes=[
                pltpu.VMEM((Y, Z, 8, W1), BF16),
                pltpu.VMEM((Y, Z, 8, W1), BF16),
                pltpu.VMEM((Z, 8, W1), BF16),
                pltpu.VMEM((Z, 8, W1), BF16),
                pltpu.VMEM((Z, 8, 128), BF16),
                pltpu.VMEM((TP, 8, 256), F32),
                pltpu.VMEM((TP, 8, 256), F32),
                pltpu.VMEM((Y * TP, 8, 256), BF16),
                pltpu.VMEM((Y, 64, W2), BF16),
                pltpu.VMEM((Y, 64, W2), BF16),
                pltpu.VMEM((Y, 256, 64), BF16),
                pltpu.VMEM((Y, FP, 64), BF16),
                pltpu.VMEM((8, 128), F32),
                pltpu.VMEM((Y, 8, 128), F32),
                pltpu.VMEM((Z, 8, W2), BF16),
                pltpu.VMEM((Z, 8, W2), BF16),
                pltpu.VMEM((Z, 8, FP), BF16),
                pltpu.VMEM((Y * TP, 8, 128), F32),
                pltpu.VMEM((Y * TP, 8, 128), F32),
                pltpu.VMEM((TP, 8, 128), BF16),
                pltpu.VMEM((256, 128), F32),
                pltpu.VMEM((64, 128), BF16),
                pltpu.SemaphoreType.DMA((PH,)),
                pltpu.SemaphoreType.DMA((PH,)),
            ],
            compiler_params=pltpu.CompilerParams(collective_id=0, has_side_effects=True),
        )(
            tokens, lengths, lengths[:, None], memory, norm_gain[None], w_query, w_key, w_value, w_outgate, w_alpha,
            w_beta, decay_log[None], decay_bias[None], head_gain[None], w_output, mlp_gain[None], w_gate, w_up, w_down,
        )
    )


def solution(mesh):
    kv, tp = "kv", "tp"
    placed = (
        P(None, kv), P(), P(kv, tp, None, None), P(kv), P(kv, tp), P(kv, tp), P(kv, tp), P(kv, tp), P(kv, None),
        P(kv, None), P(tp), P(tp), P(), P(tp, kv), P(kv), P(kv, tp), P(kv, tp), P(tp, kv),
    )
    return jax.shard_map(
        per_device,
        mesh=mesh,
        in_specs=placed,
        out_specs=(P(None, kv), P(kv, tp, None, None)),
        check_vma=False,
    )
```

```python
import jax
import jax.numpy as jnp
from jax import lax
from jax.experimental import pallas as pl
from jax.experimental.pallas import tpu as pltpu
from jax.sharding import PartitionSpec as P

MESH = pl.DeviceIdType.MESH
F32, BF16, I32 = jnp.float32, jnp.bfloat16, jnp.int32
D, DK, NEW, SEQS = 4096, 128, 4, 64
Z, Y, TP = 16, 4, 8
ROWS = SEQS * NEW
PLACES = 8 * Z
EPS = 1e-06
W1 = 640
FFY = 352
FP = 384
W2 = 2 * FP
PH = 13
S_Y, S_Z, S_M, S_C, S_H, S_G, S_A, S_F, S_O, S_WO, S_WG, S_WD, S_GN = range(PH)


def iota(shape, dim):
    return lax.broadcasted_iota(I32, shape, dim)


def mm(a, b):
    return jnp.dot(a, b, preferred_element_type=F32)


IN_NAMES = 18


def mmt(a, b):
    return lax.dot_general(a, b, (((1,), (1,)), ((), ())), preferred_element_type=F32)


def kernel(*refs):
    hbm, (out_hbm, nmem_hbm) = refs[:IN_NAMES], refs[IN_NAMES : IN_NAMES + 2]
    refs = refs[IN_NAMES + 2 :]
    own, refs = refs[:IN_NAMES], refs[IN_NAMES:]
    (
        out_ref, nmem_ref,
        part, yrecv, zs1, zr1, mrecv, cs, cr, hbuf, wgs, wgr, wob, wds, wdb, gl, gb, zs2, zr2, ab, fs, fr, ob, hct, wab,
        send, recv, load, store,
    ) = refs
    (
        tok_ref, lens_ref, mem_ref, ngain_ref, wq_ref, wk_ref, wv_ref, wg_ref, wa_ref, wb_ref,
        dlog_ref, dbias_ref, hgain_ref, wout_ref, mgain_ref, wgate_ref, wup_ref, wdown_ref,
    ) = own
    kv = lax.axis_index("kv")
    tp = lax.axis_index("tp")
    z = kv // Y
    y = kv % Y
    group = y * TP + tp

    def y_peer(k):
        return z * Y + (y + k) % Y

    def z_peer(j):
        away = 8 - (j + 1) // 2
        return (z + Z + away * (2 * (j % 2) - 1)) % Z

    barrier = pltpu.get_barrier_semaphore()

    def greet_group(j, c):
        other = (group + j) % (Y * TP)
        pl.semaphore_signal(barrier, inc=1, device_id=(z * Y + other // TP, other % TP), device_id_type=MESH)
        return c

    def greet_z(j, c):
        pl.semaphore_signal(barrier, inc=1, device_id=(z_peer(j) * Y + y, tp), device_id_type=MESH)
        return c

    loads = [pltpu.make_async_copy(hbm[k], own[k], load.at[k]) for k in range(IN_NAMES)]
    first = (0, 3, 4, 5, 6, 7, 8, 9)
    for k in first:
        loads[k].start()
    lax.fori_loop(0, Z - 1, greet_z, 0)
    lax.fori_loop(1, Y * TP, greet_group, 0)
    for k in range(IN_NAMES):
        if k not in first:
            loads[k].start()
    for k in first:
        loads[k].wait()

    def rcopy(src, dst, phase, where):
        return pltpu.make_async_remote_copy(
            src_ref=src, dst_ref=dst, send_sem=send.at[phase], recv_sem=recv.at[phase],
            device_id=where, device_id_type=MESH,
        )

    def arrived(ref, phase):
        rcopy(ref, ref, phase, (y_peer(1), tp)).wait_recv()

    def sent(ref, phase):
        rcopy(ref, ref, phase, (y_peer(1), tp)).wait_send()

    at = iota((2 * ROWS, ROWS), 0)
    row = iota((2 * ROWS, ROWS), 1)
    wanted = 16 * ((at >> 3) & 15) + 4 * (at >> 7) + (at & 3)
    turn = jnp.where(row == wanted, 1.0, 0.0).astype(BF16)
    xt = mmt(turn, tok_ref[...])
    xs = (xt * ngain_ref[...]).astype(BF16)
    wab[...] = jnp.zeros((128, 64), BF16)
    wab[64:80, :] = wa_ref[...]
    wab[80:96, :] = wb_ref[...]
    squares = jnp.sum(xt * xt, axis=1, keepdims=True)
    high = squares.astype(BF16).astype(F32)
    low = squares - high
    eye = jnp.where(iota((64, 128), 0) == iota((64, 128), 1), 1.0, 0.0).astype(BF16)
    lane = iota((2 * ROWS, 128), 1)
    extra = mmt(xs, wab[...]) + mm(xt.astype(BF16), eye)
    extra = jnp.where(lane == 96, high, jnp.where(lane == 97, low, extra))
    second = (iota((2 * ROWS, 256), 0) & 4) == 4
    left = jnp.where(second, mm(xs, wv_ref[...]), mm(xs, wq_ref[...]))
    part[:, :, :, 0:256] = left.reshape(Y, Z, 8, 256).astype(BF16)
    right = jnp.where(second, mm(xs, wg_ref[...]), mm(xs, wk_ref[...]))
    part[:, :, :, 256:512] = right.reshape(Y, Z, 8, 256).astype(BF16)
    part[:, :, :, 512:640] = extra.reshape(Y, Z, 8, 128).astype(BF16)

    for k in range(IN_NAMES):
        if k not in first:
            loads[k].wait()
    for k in range(Y):
        wgs[k, :, 0:FFY] = wgate_ref[:, FFY * k : FFY * (k + 1)]
        wgs[k, :, FFY:FP] = jnp.zeros((64, FP - FFY), BF16)
        wgs[k, :, FP : FP + FFY] = wup_ref[:, FFY * k : FFY * (k + 1)]
        wgs[k, :, FP + FFY : W2] = jnp.zeros((64, FP - FFY), BF16)
        wds[k, :, 0:FFY] = wdown_ref[:, FFY * k : FFY * (k + 1)]
        wds[k, :, FFY:FP] = jnp.zeros((64, FP - FFY), BF16)
    gl[...] = jnp.zeros((8, 128), F32) + jnp.concatenate([mgain_ref[...], mgain_ref[...]], axis=1)

    pl.semaphore_wait(barrier, Z - 1 + Y * TP - 1)

    for k in range(1, Y):
        peer = y_peer(k)
        rcopy(part.at[peer % Y], yrecv.at[y], S_Y, (peer, tp)).start()
    for k in range(1, Y):
        peer = y_peer(k)
        rcopy(wout_ref, wob.at[y], S_WO, (peer, tp)).start()
        rcopy(wgs.at[peer % Y], wgr.at[y], S_WG, (peer, tp)).start()
        rcopy(wds.at[peer % Y], wdb.at[y], S_WD, (peer, tp)).start()
        rcopy(gl, gb.at[y], S_GN, (peer, tp)).start()

    yrecv[y] = part[y]
    wob[y] = wout_ref[...]
    wgr[y] = wgs[y]
    wdb[y] = wds[y]
    gb[y] = gl[...]

    seq = iota((SEQS, ROWS), 0)
    lens8 = jnp.concatenate([lens_ref[...], lens_ref[...]], axis=1).astype(F32) + jnp.zeros((8, 128), F32)
    lens = lens8.T[0:SEQS, 0:1].astype(I32) + jnp.zeros((SEQS, ROWS), I32)
    place = iota((PLACES, ROWS), 0)

    def chooser(seq_of, slot):
        mine = jnp.sum(jnp.where(seq == seq_of, lens, 0), axis=0, keepdims=True)
        before = jnp.sum(jnp.where(seq < seq_of, lens, 0), axis=0, keepdims=True)
        slot = slot[0:1]
        index = before + slot
        chunk = (index * 9363) >> 16
        goes = jnp.where(slot < mine, index + chunk, -1)
        return jnp.where(place == goes, 1.0, 0.0).astype(BF16)

    col = iota((SEQS, ROWS), 1)
    pick = chooser(4 * ((col >> 2) & 15) + (col >> 6), col & 3)
    give = chooser(col >> 2, col & 3)

    arrived(yrecv.at[0:3], S_Y)
    total = yrecv[0].astype(F32)
    for k in range(1, Y):
        total = total + yrecv[k].astype(F32)
    zs1[...] = total.astype(BF16)

    def send_z1(j, c):
        to = z_peer(j)
        rcopy(zs1.at[to], zr1.at[z], S_Z, (to * Y + y, tp)).start()
        return c

    lax.fori_loop(0, Z - 1, send_z1, 0)
    zr1[z] = zs1[z]
    arrived(zr1.at[0 : Z - 1], S_Z)

    mine = jnp.sum(zr1[...].astype(F32), axis=0)
    lane8 = iota((8, 128), 1)
    ext = mine[:, 512:640]

    def lane_of(values, where):
        return jnp.sum(jnp.where(lane8 == where, values, 0.0), axis=1, keepdims=True)

    rstd = lax.rsqrt((lane_of(ext, 96) + lane_of(ext, 97)) / D + EPS)
    main = (mine[:, 0:512] * rstd).astype(BF16).astype(F32)
    ext = ext * rstd
    length = jnp.sum(jnp.where(iota((1, SEQS), 1) == kv, lens_ref[...], 0), axis=1, keepdims=True)
    live = iota((8, 1), 0) < length
    rows = []
    for h in range(2):
        alpha = lane_of(ext, 64 + 2 * tp + h)
        beta = jax.nn.sigmoid(lane_of(ext, 80 + 2 * tp + h))
        shifted = alpha + dbias_ref[:, h : h + 1]
        soft = jnp.maximum(shifted, 0.0) + jnp.log1p(jnp.exp(-jnp.abs(shifted)))
        rate = jnp.exp(jnp.zeros((8, 1), F32) + dlog_ref[:, h : h + 1])
        decay = jnp.exp(jnp.where(live, -rate * soft, 0.0))
        beta = jnp.where(live, beta, 0.0)
        q8 = main[:, 128 * h : 128 * h + 128]
        k8 = main[:, 256 + 128 * h : 384 + 128 * h]
        q8 = q8 * lax.rsqrt(jnp.sum(q8 * q8, axis=1, keepdims=True) + EPS) * DK**-0.5
        k8 = k8 * lax.rsqrt(jnp.sum(k8 * k8, axis=1, keepdims=True) + EPS)
        qt, kt = q8.T, k8.T
        memory = mem_ref[0, h]
        for t in range(NEW):
            kcol = kt[:, t : t + 1]
            memory = memory * decay[t : t + 1]
            guess = jnp.sum(memory * kcol, axis=0, keepdims=True)
            fix = beta[t : t + 1] * (main[4 + t : 5 + t, 128 * h : 128 * h + 128] - guess)
            memory = memory + kcol * fix
            rows.append(jnp.sum(memory * qt[:, t : t + 1], axis=0, keepdims=True))
        nmem_ref[0, h] = memory
    keep = pltpu.make_async_copy(nmem_ref, nmem_hbm, store.at[0])
    keep.start()
    attended = jnp.concatenate(rows, axis=0)
    attended = attended * lax.rsqrt(jnp.mean(attended * attended, axis=1, keepdims=True) + EPS)
    gates = jnp.concatenate([main[4:8, 256:384], main[4:8, 384:512]], axis=0)
    mixed = attended * hgain_ref[...] * (gates * jax.nn.sigmoid(gates))
    mrecv[z] = mixed.astype(BF16)

    def send_m(j, c):
        rcopy(mrecv.at[z], mrecv.at[z], S_M, (z_peer(j) * Y + y, tp)).start()
        return c

    lax.fori_loop(0, Z - 1, send_m, 0)
    arrived(wob.at[0:3], S_WO)
    wo = wob[...].reshape(256, 256)
    arrived(gb.at[0:3], S_GN)
    low_lane = iota((1, 128), 1) < 64
    gain = jnp.concatenate(
        [jnp.where(low_lane, gb[0, 0:1], gb[1, 0:1]), jnp.where(low_lane, gb[2, 0:1], gb[3, 0:1])], axis=1
    )
    low_half = iota((8, 128), 0) < 4

    def kept(k):
        return jnp.where(
            low_half, yrecv[k, 2 * tp, :, 512:640].astype(F32), yrecv[k, 2 * tp + 1, :, 512:640].astype(F32)
        )

    residual = jnp.concatenate(
        [
            jnp.where(low_lane, kept(0), pltpu.roll(kept(1), 64, 1)),
            jnp.where(low_lane, kept(2), pltpu.roll(kept(3), 64, 1)),
        ],
        axis=1,
    )
    arrived(mrecv.at[0 : Z - 1], S_M)

    heads = mrecv[...].astype(F32).reshape(8 * Z, 128).astype(BF16)
    first_head = (iota((8 * Z, 256), 0) & 4) == 0
    terms = jnp.where(first_head, mmt(heads, wo[:, 0:128]), mmt(heads, wo[:, 128:256]))
    terms = terms.reshape(TP, 2, 8, 256)
    even, odd = terms[:, 0], terms[:, 1]
    even = even + jnp.concatenate([even[:, 4:8], even[:, 0:4]], axis=1)
    odd = odd + jnp.concatenate([odd[:, 4:8], odd[:, 0:4]], axis=1)
    cs[...] = jnp.where((iota((TP, 8, 256), 1) & 4) == 0, even, odd)

    def send_c(j, c):
        to = (tp + j) % TP
        rcopy(cs.at[to], cr.at[tp], S_C, (kv, to)).start()
        return c

    lax.fori_loop(1, TP, send_c, 0)
    cr[tp] = cs[tp]
    arrived(cr.at[0 : TP - 1], S_C)
    hbuf[group] = (residual + jnp.sum(cr[...], axis=0)).astype(BF16)

    def send_h(j, c):
        other = (group + j) % (Y * TP)
        rcopy(hbuf.at[group], hbuf.at[group], S_H, (z * Y + other // TP, other % TP)).start()
        return c

    lax.fori_loop(1, Y * TP, send_h, 0)
    arrived(wgr.at[0:3], S_WG)
    arrived(hbuf.at[0 : Y * TP - 1], S_H)

    hidden = mm(pick, hbuf[...].astype(F32).reshape(ROWS, 256).astype(BF16))
    hscaled = (hidden * gain).astype(BF16)
    products = mm(hscaled, wgr[...].reshape(256, W2))
    squares2 = jnp.sum(hidden * hidden, axis=1, keepdims=True)
    high2 = squares2.astype(BF16).astype(F32)
    low2 = squares2 - high2
    lane2 = iota((PLACES, W2), 1)
    products = jnp.where(lane2 == FFY, high2, jnp.where(lane2 == FFY + 1, low2, products))
    zs2[...] = products.reshape(Z, 8, W2).astype(BF16)

    def send_g(j, c):
        to = z_peer(j)
        rcopy(zs2.at[to], zr2.at[z], S_G, (to * Y + y, tp)).start()
        return c

    lax.fori_loop(0, Z - 1, send_g, 0)
    zr2[z] = zs2[z]
    hct[...] = hidden.T
    arrived(wdb.at[0:3], S_WD)
    arrived(zr2.at[0 : Z - 1], S_G)
    summed = jnp.sum(zr2[...].astype(F32), axis=0)
    lane3 = iota((8, FP), 1)
    gate, up = summed[:, 0:FP], summed[:, FP:W2]
    total2 = jnp.sum(jnp.where((lane3 == FFY) | (lane3 == FFY + 1), gate, 0.0), axis=1, keepdims=True)
    rstd2 = lax.rsqrt(total2 / D + EPS)
    gate = jnp.where(lane3 < FFY, gate, 0.0) * rstd2
    ab[z] = (gate * jax.nn.sigmoid(gate) * (up * rstd2)).astype(BF16)

    def send_a(j, c):
        rcopy(ab.at[z], ab.at[z], S_A, (z_peer(j) * Y + y, tp)).start()
        return c

    lax.fori_loop(0, Z - 1, send_a, 0)
    arrived(ab.at[0 : Z - 1], S_A)

    active = ab[...].astype(F32).reshape(PLACES, FP).astype(BF16)
    fs[...] = mmt(wdb[...].reshape(256, FP), active).reshape(Y * TP, 8, 128)

    def send_f(j, c):
        other = (group + j) % (Y * TP)
        rcopy(fs.at[other], fr.at[group], S_F, (z * Y + other // TP, other % TP)).start()
        return c

    lax.fori_loop(1, Y * TP, send_f, 0)
    fr[group] = fs[group]
    arrived(fr.at[0 : Y * TP - 1], S_F)
    ended = jnp.sum(fr[...], axis=0) + hct[pl.ds(pl.multiple_of(8 * group, 8), 8), :]
    ob[tp] = ended.astype(BF16)

    def send_o(j, c):
        rcopy(ob.at[tp], ob.at[tp], S_O, (kv, (tp + j) % TP)).start()
        return c

    lax.fori_loop(1, TP, send_o, 0)
    arrived(ob.at[0 : TP - 1], S_O)
    final = ob[...].astype(F32).reshape(64, PLACES).astype(BF16)
    out_ref[...] = mm(final, give).astype(BF16)
    result = pltpu.make_async_copy(out_ref, out_hbm, store.at[1])
    result.start()

    for ref, phase in (
        (yrecv.at[0:3], S_Y), (zr1.at[0 : Z - 1], S_Z), (mrecv.at[0 : Z - 1], S_M), (cr.at[0 : TP - 1], S_C),
        (hbuf.at[0 : Y * TP - 1], S_H), (zr2.at[0 : Z - 1], S_G), (ab.at[0 : Z - 1], S_A),
        (fr.at[0 : Y * TP - 1], S_F), (ob.at[0 : TP - 1], S_O), (wob.at[0:3], S_WO), (wgr.at[0:3], S_WG),
        (wdb.at[0:3], S_WD), (gb.at[0:3], S_GN),
    ):
        sent(ref, phase)
    keep.wait()
    result.wait()


def per_device(
    tokens, lengths, memory, norm_gain, w_query, w_key, w_value, w_outgate, w_alpha, w_beta, decay_log, decay_bias,
    head_gain, w_output, mlp_gain, w_gate, w_up, w_down,
):
    inputs = (
        tokens.T, lengths[None], memory, norm_gain[None], w_query, w_key, w_value, w_outgate, w_alpha.T, w_beta.T,
        decay_log[None], decay_bias[None], head_gain[None], w_output.T, mlp_gain[None], w_gate, w_up, w_down.T,
    )
    outputs = (jax.ShapeDtypeStruct((64, ROWS), BF16), jax.ShapeDtypeStruct(memory.shape, F32))
    shapes = [((Y, Z, 8, W1), BF16)] * 2 + [((Z, 8, W1), BF16)] * 2 + [
        ((Z, 8, 128), BF16),
        ((TP, 8, 256), F32),
        ((TP, 8, 256), F32),
        ((Y * TP, 8, 256), BF16),
        ((Y, 64, W2), BF16),
        ((Y, 64, W2), BF16),
        ((Y, 64, 256), BF16),
        ((Y, 64, FP), BF16),
        ((Y, 64, FP), BF16),
        ((8, 128), F32),
        ((Y, 8, 128), F32),
        ((Z, 8, W2), BF16),
        ((Z, 8, W2), BF16),
        ((Z, 8, FP), BF16),
        ((Y * TP, 8, 128), F32),
        ((Y * TP, 8, 128), F32),
        ((TP, 8, 128), BF16),
        ((256, 128), F32),
        ((128, 64), BF16),
    ]
    result, new_memory = pl.pallas_call(
        kernel,
        out_shape=outputs,
        in_specs=[pl.BlockSpec(memory_space=pl.ANY)] * IN_NAMES,
        out_specs=tuple([pl.BlockSpec(memory_space=pl.ANY)] * 2),
        scratch_shapes=[pltpu.VMEM(a.shape, a.dtype) for a in inputs + outputs]
        + [pltpu.VMEM(*shape) for shape in shapes]
        + [
            pltpu.SemaphoreType.DMA((PH,)),
            pltpu.SemaphoreType.DMA((PH,)),
            pltpu.SemaphoreType.DMA((IN_NAMES,)),
            pltpu.SemaphoreType.DMA((2,)),
        ],
        compiler_params=pltpu.CompilerParams(collective_id=0, has_side_effects=True),
    )(*inputs)
    return (result.T, new_memory)


def solution(mesh):
    kv, tp = "kv", "tp"
    placed = (
        P(None, kv), P(), P(kv, tp, None, None), P(kv), P(kv, tp), P(kv, tp), P(kv, tp), P(kv, tp), P(kv, None),
        P(kv, None), P(tp), P(tp), P(), P(tp, kv), P(kv), P(kv, tp), P(kv, tp), P(tp, kv),
    )
    return jax.shard_map(
        per_device,
        mesh=mesh,
        in_specs=placed,
        out_specs=(P(None, kv), P(kv, tp, None, None)),
        check_vma=False,
    )
```

```python
import jax
import jax.numpy as jnp
from jax import lax
from jax.experimental import pallas as pl
from jax.experimental.pallas import tpu as pltpu
from jax.sharding import PartitionSpec as P

MESH = pl.DeviceIdType.MESH
F32, BF16, I32 = jnp.float32, jnp.bfloat16, jnp.int32
D, DK, NEW, SEQS = 4096, 128, 4, 64
Z, Y, TP = 16, 4, 8
ROWS = SEQS * NEW
PLACES = 8 * Z
EPS = 1e-06
W1 = 640
FFY = 352
FP = 384
W2 = 2 * FP
PH = 16
S_Z, S_M, S_C, S_H, S_G, S_A, S_F, S_O, S_WO, S_WG, S_WD, S_GN, S_Y = range(PH - 3)
PARTS = 4
SLOTS = Z // PARTS


def iota(shape, dim):
    return lax.broadcasted_iota(I32, shape, dim)


def mm(a, b):
    return jnp.dot(a, b, preferred_element_type=F32)


IN_NAMES = 18


def mmt(a, b):
    return lax.dot_general(a, b, (((1,), (1,)), ((), ())), preferred_element_type=F32)


def kernel(*refs):
    hbm, (out_hbm, nmem_hbm) = refs[:IN_NAMES], refs[IN_NAMES : IN_NAMES + 2]
    refs = refs[IN_NAMES + 2 :]
    own, refs = refs[:IN_NAMES], refs[IN_NAMES:]
    (
        out_ref, nmem_ref,
        part, yrecv, zs1, zr1, mrecv, cs, cr, hbuf, wgs, wgr, wob, wds, wdb, gl, gb, zs2, zr2, ab, fs, fr, ob, hct, wab,
        send, recv, load, store, known,
    ) = refs
    (
        tok_ref, lens_ref, mem_ref, ngain_ref, wq_ref, wk_ref, wv_ref, wg_ref, wa_ref, wb_ref,
        dlog_ref, dbias_ref, hgain_ref, wout_ref, mgain_ref, wgate_ref, wup_ref, wdown_ref,
    ) = own
    kv = lax.axis_index("kv")
    tp = lax.axis_index("tp")
    z = kv // Y
    y = kv % Y
    group = y * TP + tp

    def y_peer(k):
        return z * Y + (y + k) % Y

    def z_peer(j):
        away = 8 - (j + 1) // 2
        return (z + Z + away * (2 * (j % 2) - 1)) % Z

    barrier = pltpu.get_barrier_semaphore()

    def greet_group(j, c):
        other = (group + j) % (Y * TP)
        pl.semaphore_signal(barrier, inc=1, device_id=(z * Y + other // TP, other % TP), device_id_type=MESH)
        return c

    def z_near(k):
        return (((z + k + Z) % Z) * Y + y, tp)

    loads = [pltpu.make_async_copy(hbm[k], own[k], load.at[k]) for k in range(IN_NAMES)]
    first = (0, 3, 4, 5, 6, 7, 8, 9)
    for k in first:
        loads[k].start()
    for k in (1, -1):
        pl.semaphore_signal(barrier, inc=1, device_id=z_near(k), device_id_type=MESH)
    lax.fori_loop(1, Y * TP, greet_group, 0)
    for k in range(IN_NAMES):
        if k not in first:
            loads[k].start()
    for k in first:
        loads[k].wait()

    def rcopy(src, dst, phase, where):
        return pltpu.make_async_remote_copy(
            src_ref=src, dst_ref=dst, send_sem=send.at[phase], recv_sem=recv.at[phase],
            device_id=where, device_id_type=MESH,
        )

    def arrived(ref, phase):
        rcopy(ref, ref, phase, (y_peer(1), tp)).wait_recv()

    def sent(ref, phase):
        rcopy(ref, ref, phase, (y_peer(1), tp)).wait_send()

    at = iota((2 * ROWS, ROWS), 0)
    row = iota((2 * ROWS, ROWS), 1)
    slot = (at >> 3) & 15
    toward = (z + Z + (8 - ((slot + 1) >> 1)) * (2 * (slot & 1) - 1)) & 15
    wanted = 16 * toward + 4 * (at >> 7) + (at & 3)
    turn = jnp.where(row == wanted, 1.0, 0.0).astype(BF16)
    xt = mmt(turn, tok_ref[...])
    xs = (xt * ngain_ref[...]).astype(BF16)
    wab[...] = jnp.zeros((128, 64), BF16)
    wab[64:80, :] = wa_ref[...]
    wab[80:96, :] = wb_ref[...]
    squares = jnp.sum(xt * xt, axis=1, keepdims=True)
    high = squares.astype(BF16).astype(F32)
    low = squares - high
    eye = jnp.where(iota((64, 128), 0) == iota((64, 128), 1), 1.0, 0.0).astype(BF16)
    lane = iota((2 * ROWS, 128), 1)
    extra = mmt(xs, wab[...]) + mm(xt.astype(BF16), eye)
    extra = jnp.where(lane == 96, high, jnp.where(lane == 97, low, extra))
    second = (iota((2 * ROWS, 256), 0) & 4) == 4
    left = jnp.where(second, mm(xs, wv_ref[...]), mm(xs, wq_ref[...]))
    part[:, :, :, 0:256] = left.reshape(Y, Z, 8, 256).astype(BF16)
    right = jnp.where(second, mm(xs, wg_ref[...]), mm(xs, wk_ref[...]))
    part[:, :, :, 256:512] = right.reshape(Y, Z, 8, 256).astype(BF16)
    part[:, :, :, 512:640] = extra.reshape(Y, Z, 8, 128).astype(BF16)

    for k in range(IN_NAMES):
        if k not in first:
            loads[k].wait()
    for k in range(Y):
        wgs[k, :, 0:FFY] = wgate_ref[:, FFY * k : FFY * (k + 1)]
        wgs[k, :, FFY:FP] = jnp.zeros((64, FP - FFY), BF16)
        wgs[k, :, FP : FP + FFY] = wup_ref[:, FFY * k : FFY * (k + 1)]
        wgs[k, :, FP + FFY : W2] = jnp.zeros((64, FP - FFY), BF16)
        wds[k, :, 0:FFY] = wdown_ref[:, FFY * k : FFY * (k + 1)]
        wds[k, :, FFY:FP] = jnp.zeros((64, FP - FFY), BF16)
    gl[...] = jnp.zeros((8, 128), F32) + jnp.concatenate([mgain_ref[...], mgain_ref[...]], axis=1)

    pl.semaphore_wait(barrier, 2 + Y * TP - 1)

    def tell(n):
        for k in (1 << n, -(1 << n)):
            pl.semaphore_signal(known.at[n], inc=1, device_id=z_near(k), device_id_type=MESH)

    tell(0)
    for c in range(PARTS):
        some = pl.ds(SLOTS * c, SLOTS)
        for k in range(1, Y):
            peer = y_peer(k)
            rcopy(part.at[peer % Y, some], yrecv.at[y, some], S_Y + c, (peer, tp)).start()
    for k in range(1, Y):
        peer = y_peer(k)
        rcopy(wout_ref, wob.at[y], S_WO, (peer, tp)).start()
        rcopy(wgs.at[peer % Y], wgr.at[y], S_WG, (peer, tp)).start()
        rcopy(wds.at[peer % Y], wdb.at[y], S_WD, (peer, tp)).start()
        rcopy(gl, gb.at[y], S_GN, (peer, tp)).start()

    pl.semaphore_wait(known.at[0], 2)
    tell(1)
    yrecv[y] = part[y]
    wob[y] = wout_ref[...]
    wgr[y] = wgs[y]
    wdb[y] = wds[y]
    gb[y] = gl[...]

    pl.semaphore_wait(known.at[1], 2)
    tell(2)

    def send_z1(j, c):
        to = z_peer(j)
        rcopy(zs1.at[j], zr1.at[z], S_Z, (to * Y + y, tp)).start()
        return c

    pl.semaphore_wait(known.at[2], 2)
    for c in range(PARTS):
        low, high_slot = SLOTS * c, SLOTS * (c + 1)
        arrived(yrecv.at[0:3, low:high_slot], S_Y + c)
        total = yrecv[0, low:high_slot].astype(F32)
        for k in range(1, Y):
            total = total + yrecv[k, low:high_slot].astype(F32)
        zs1[low:high_slot] = total.astype(BF16)
        lax.fori_loop(low, min(high_slot, Z - 1), send_z1, 0)
    zr1[z] = zs1[Z - 1]

    seq = iota((SEQS, ROWS), 0)
    lens8 = jnp.concatenate([lens_ref[...], lens_ref[...]], axis=1).astype(F32) + jnp.zeros((8, 128), F32)
    lens = lens8.T[0:SEQS, 0:1].astype(I32) + jnp.zeros((SEQS, ROWS), I32)
    place = iota((PLACES, ROWS), 0)

    def chooser(seq_of, slot):
        mine = jnp.sum(jnp.where(seq == seq_of, lens, 0), axis=0, keepdims=True)
        before = jnp.sum(jnp.where(seq < seq_of, lens, 0), axis=0, keepdims=True)
        slot = slot[0:1]
        index = before + slot
        chunk = (index * 9363) >> 16
        goes = jnp.where(slot < mine, index + chunk, -1)
        return jnp.where(place == goes, 1.0, 0.0).astype(BF16)

    col = iota((SEQS, ROWS), 1)
    pick = chooser(4 * ((col >> 2) & 15) + (col >> 6), col & 3)
    give = chooser(col >> 2, col & 3)

    arrived(zr1.at[0 : Z - 1], S_Z)

    mine = jnp.sum(zr1[...].astype(F32), axis=0)
    lane8 = iota((8, 128), 1)
    ext = mine[:, 512:640]

    def lane_of(values, where):
        return jnp.sum(jnp.where(lane8 == where, values, 0.0), axis=1, keepdims=True)

    rstd = lax.rsqrt((lane_of(ext, 96) + lane_of(ext, 97)) / D + EPS)
    main = (mine[:, 0:512] * rstd).astype(BF16).astype(F32)
    ext = ext * rstd
    length = jnp.sum(jnp.where(iota((1, SEQS), 1) == kv, lens_ref[...], 0), axis=1, keepdims=True)
    live = iota((8, 1), 0) < length
    rows = []
    for h in range(2):
        alpha = lane_of(ext, 64 + 2 * tp + h)
        beta = jax.nn.sigmoid(lane_of(ext, 80 + 2 * tp + h))
        shifted = alpha + dbias_ref[:, h : h + 1]
        soft = jnp.maximum(shifted, 0.0) + jnp.log1p(jnp.exp(-jnp.abs(shifted)))
        rate = jnp.exp(jnp.zeros((8, 1), F32) + dlog_ref[:, h : h + 1])
        decay = jnp.exp(jnp.where(live, -rate * soft, 0.0))
        beta = jnp.where(live, beta, 0.0)
        q8 = main[:, 128 * h : 128 * h + 128]
        k8 = main[:, 256 + 128 * h : 384 + 128 * h]
        q8 = q8 * lax.rsqrt(jnp.sum(q8 * q8, axis=1, keepdims=True) + EPS) * DK**-0.5
        k8 = k8 * lax.rsqrt(jnp.sum(k8 * k8, axis=1, keepdims=True) + EPS)
        qt, kt = q8.T, k8.T
        memory = mem_ref[0, h]
        for t in range(NEW):
            kcol = kt[:, t : t + 1]
            memory = memory * decay[t : t + 1]
            guess = jnp.sum(memory * kcol, axis=0, keepdims=True)
            fix = beta[t : t + 1] * (main[4 + t : 5 + t, 128 * h : 128 * h + 128] - guess)
            memory = memory + kcol * fix
            rows.append(jnp.sum(memory * qt[:, t : t + 1], axis=0, keepdims=True))
        nmem_ref[0, h] = memory
    keep = pltpu.make_async_copy(nmem_ref, nmem_hbm, store.at[0])
    keep.start()
    attended = jnp.concatenate(rows, axis=0)
    attended = attended * lax.rsqrt(jnp.mean(attended * attended, axis=1, keepdims=True) + EPS)
    gates = jnp.concatenate([main[4:8, 256:384], main[4:8, 384:512]], axis=0)
    mixed = attended * hgain_ref[...] * (gates * jax.nn.sigmoid(gates))
    mrecv[z] = mixed.astype(BF16)

    def send_m(j, c):
        rcopy(mrecv.at[z], mrecv.at[z], S_M, (z_peer(j) * Y + y, tp)).start()
        return c

    lax.fori_loop(0, Z - 1, send_m, 0)
    arrived(wob.at[0:3], S_WO)
    wo = wob[...].reshape(256, 256)
    arrived(gb.at[0:3], S_GN)
    low_lane = iota((1, 128), 1) < 64
    gain = jnp.concatenate(
        [jnp.where(low_lane, gb[0, 0:1], gb[1, 0:1]), jnp.where(low_lane, gb[2, 0:1], gb[3, 0:1])], axis=1
    )
    low_half = iota((8, 128), 0) < 4

    def slot_of(where):
        away = (where - z + Z) % Z
        return (1 - away // 8) * (15 - 2 * away) + (away // 8) * (2 * away - 16)

    def kept(k):
        return jnp.where(
            low_half,
            yrecv[k, slot_of(2 * tp), :, 512:640].astype(F32),
            yrecv[k, slot_of(2 * tp + 1), :, 512:640].astype(F32),
        )

    residual = jnp.concatenate(
        [
            jnp.where(low_lane, kept(0), pltpu.roll(kept(1), 64, 1)),
            jnp.where(low_lane, kept(2), pltpu.roll(kept(3), 64, 1)),
        ],
        axis=1,
    )
    arrived(mrecv.at[0 : Z - 1], S_M)

    heads = mrecv[...].astype(F32).reshape(8 * Z, 128).astype(BF16)
    first_head = (iota((8 * Z, 256), 0) & 4) == 0
    terms = jnp.where(first_head, mmt(heads, wo[:, 0:128]), mmt(heads, wo[:, 128:256]))
    terms = terms.reshape(TP, 2, 8, 256)
    even, odd = terms[:, 0], terms[:, 1]
    even = even + jnp.concatenate([even[:, 4:8], even[:, 0:4]], axis=1)
    odd = odd + jnp.concatenate([odd[:, 4:8], odd[:, 0:4]], axis=1)
    cs[...] = jnp.where((iota((TP, 8, 256), 1) & 4) == 0, even, odd).astype(BF16)

    def send_c(j, c):
        to = (tp + j) % TP
        rcopy(cs.at[to], cr.at[tp], S_C, (kv, to)).start()
        return c

    lax.fori_loop(1, TP, send_c, 0)
    cr[tp] = cs[tp]
    arrived(cr.at[0 : TP - 1], S_C)
    hbuf[group] = (residual + jnp.sum(cr[...].astype(F32), axis=0)).astype(BF16)

    def send_h(j, c):
        other = (group + j) % (Y * TP)
        rcopy(hbuf.at[group], hbuf.at[group], S_H, (z * Y + other // TP, other % TP)).start()
        return c

    lax.fori_loop(1, Y * TP, send_h, 0)
    arrived(wgr.at[0:3], S_WG)
    arrived(hbuf.at[0 : Y * TP - 1], S_H)

    hidden = mm(pick, hbuf[...].astype(F32).reshape(ROWS, 256).astype(BF16))
    hscaled = (hidden * gain).astype(BF16)
    products = mm(hscaled, wgr[...].reshape(256, W2))
    squares2 = jnp.sum(hidden * hidden, axis=1, keepdims=True)
    high2 = squares2.astype(BF16).astype(F32)
    low2 = squares2 - high2
    lane2 = iota((PLACES, W2), 1)
    products = jnp.where(lane2 == FFY, high2, jnp.where(lane2 == FFY + 1, low2, products))
    zs2[...] = products.reshape(Z, 8, W2).astype(BF16)

    def send_g(j, c):
        to = z_peer(j)
        rcopy(zs2.at[to], zr2.at[z], S_G, (to * Y + y, tp)).start()
        return c

    lax.fori_loop(0, Z - 1, send_g, 0)
    zr2[z] = zs2[z]
    hct[...] = hidden.T
    arrived(wdb.at[0:3], S_WD)
    arrived(zr2.at[0 : Z - 1], S_G)
    summed = jnp.sum(zr2[...].astype(F32), axis=0)
    lane3 = iota((8, FP), 1)
    gate, up = summed[:, 0:FP], summed[:, FP:W2]
    total2 = jnp.sum(jnp.where((lane3 == FFY) | (lane3 == FFY + 1), gate, 0.0), axis=1, keepdims=True)
    rstd2 = lax.rsqrt(total2 / D + EPS)
    gate = jnp.where(lane3 < FFY, gate, 0.0) * rstd2
    ab[z] = (gate * jax.nn.sigmoid(gate) * (up * rstd2)).astype(BF16)

    def send_a(j, c):
        rcopy(ab.at[z], ab.at[z], S_A, (z_peer(j) * Y + y, tp)).start()
        return c

    lax.fori_loop(0, Z - 1, send_a, 0)
    arrived(ab.at[0 : Z - 1], S_A)

    active = ab[...].astype(F32).reshape(PLACES, FP).astype(BF16)
    fs[...] = mmt(wdb[...].reshape(256, FP), active).reshape(Y * TP, 8, 128).astype(BF16)

    def send_f(j, c):
        other = (group + j) % (Y * TP)
        rcopy(fs.at[other], fr.at[group], S_F, (z * Y + other // TP, other % TP)).start()
        return c

    lax.fori_loop(1, Y * TP, send_f, 0)
    fr[group] = fs[group]
    arrived(fr.at[0 : Y * TP - 1], S_F)
    ended = jnp.sum(fr[...].astype(F32), axis=0) + hct[pl.ds(pl.multiple_of(8 * group, 8), 8), :]
    ob[tp] = ended.astype(BF16)

    def send_o(j, c):
        rcopy(ob.at[tp], ob.at[tp], S_O, (kv, (tp + j) % TP)).start()
        return c

    lax.fori_loop(1, TP, send_o, 0)
    arrived(ob.at[0 : TP - 1], S_O)
    final = ob[...].astype(F32).reshape(64, PLACES).astype(BF16)
    out_ref[...] = mm(final, give).astype(BF16)
    result = pltpu.make_async_copy(out_ref, out_hbm, store.at[1])
    result.start()

    for ref, phase in (
        (zr1.at[0 : Z - 1], S_Z), (mrecv.at[0 : Z - 1], S_M), (cr.at[0 : TP - 1], S_C),
        (hbuf.at[0 : Y * TP - 1], S_H), (zr2.at[0 : Z - 1], S_G), (ab.at[0 : Z - 1], S_A),
        (fr.at[0 : Y * TP - 1], S_F), (ob.at[0 : TP - 1], S_O), (wob.at[0:3], S_WO), (wgr.at[0:3], S_WG),
        (wdb.at[0:3], S_WD), (gb.at[0:3], S_GN),
    ):
        sent(ref, phase)
    for c in range(PARTS):
        sent(yrecv.at[0:3, 0:SLOTS], S_Y + c)
    keep.wait()
    result.wait()


def per_device(
    tokens, lengths, memory, norm_gain, w_query, w_key, w_value, w_outgate, w_alpha, w_beta, decay_log, decay_bias,
    head_gain, w_output, mlp_gain, w_gate, w_up, w_down,
):
    inputs = (
        tokens.T, lengths[None], memory, norm_gain[None], w_query, w_key, w_value, w_outgate, w_alpha.T, w_beta.T,
        decay_log[None], decay_bias[None], head_gain[None], w_output.T, mlp_gain[None], w_gate, w_up, w_down.T,
    )
    outputs = (jax.ShapeDtypeStruct((64, ROWS), BF16), jax.ShapeDtypeStruct(memory.shape, F32))
    shapes = [((Y, Z, 8, W1), BF16)] * 2 + [((Z, 8, W1), BF16)] * 2 + [
        ((Z, 8, 128), BF16),
        ((TP, 8, 256), BF16),
        ((TP, 8, 256), BF16),
        ((Y * TP, 8, 256), BF16),
        ((Y, 64, W2), BF16),
        ((Y, 64, W2), BF16),
        ((Y, 64, 256), BF16),
        ((Y, 64, FP), BF16),
        ((Y, 64, FP), BF16),
        ((8, 128), F32),
        ((Y, 8, 128), F32),
        ((Z, 8, W2), BF16),
        ((Z, 8, W2), BF16),
        ((Z, 8, FP), BF16),
        ((Y * TP, 8, 128), BF16),
        ((Y * TP, 8, 128), BF16),
        ((TP, 8, 128), BF16),
        ((256, 128), F32),
        ((128, 64), BF16),
    ]
    result, new_memory = pl.pallas_call(
        kernel,
        out_shape=outputs,
        in_specs=[pl.BlockSpec(memory_space=pl.ANY)] * IN_NAMES,
        out_specs=tuple([pl.BlockSpec(memory_space=pl.ANY)] * 2),
        scratch_shapes=[pltpu.VMEM(a.shape, a.dtype) for a in inputs + outputs]
        + [pltpu.VMEM(*shape) for shape in shapes]
        + [
            pltpu.SemaphoreType.DMA((PH,)),
            pltpu.SemaphoreType.DMA((PH,)),
            pltpu.SemaphoreType.DMA((IN_NAMES,)),
            pltpu.SemaphoreType.DMA((2,)),
            pltpu.SemaphoreType.REGULAR((3,)),
        ],
        compiler_params=pltpu.CompilerParams(collective_id=0, has_side_effects=True),
    )(*inputs)
    return (result.T, new_memory)


def solution(mesh):
    kv, tp = "kv", "tp"
    placed = (
        P(None, kv), P(), P(kv, tp, None, None), P(kv), P(kv, tp), P(kv, tp), P(kv, tp), P(kv, tp), P(kv, None),
        P(kv, None), P(tp), P(tp), P(), P(tp, kv), P(kv), P(kv, tp), P(kv, tp), P(tp, kv),
    )
    return jax.shard_map(
        per_device,
        mesh=mesh,
        in_specs=placed,
        out_specs=(P(None, kv), P(kv, tp, None, None)),
        check_vma=False,
    )
```

```python
import jax
import jax.numpy as jnp
from jax import lax
from jax.experimental import pallas as pl
from jax.experimental.pallas import tpu as pltpu
from jax.sharding import PartitionSpec as P

MESH = pl.DeviceIdType.MESH
F32, BF16, I32 = jnp.float32, jnp.bfloat16, jnp.int32
D, DK, NEW, SEQS = 4096, 128, 4, 64
Z, Y, X, TP = 16, 4, 4, 8
ROWS = SEQS * NEW
PLACES = 8 * Z
EPS = 1e-06
W1 = 640
FFY = 352
FP = 384
W2 = 2 * FP
PH = 16
S_Z, S_M, S_C, S_H, S_G, S_A, S_F, S_O, S_WO, S_WG, S_WD, S_GN, S_Y = range(PH - 3)
PARTS = 4
SLOTS = Z // PARTS


def iota(shape, dim):
    return lax.broadcasted_iota(I32, shape, dim)


def mm(a, b):
    return jnp.dot(a, b, preferred_element_type=F32)


IN_NAMES = 18


def mmt(a, b):
    return lax.dot_general(a, b, (((1,), (1,)), ((), ())), preferred_element_type=F32)


def kernel(*refs):
    hbm, (out_ref, nmem_ref) = refs[:IN_NAMES], refs[IN_NAMES : IN_NAMES + 2]
    refs = refs[IN_NAMES + 2 :]
    own, refs = refs[:IN_NAMES], refs[IN_NAMES:]
    (
        part, yrecv, zs1, zr1, mrecv, cs, cr, hbuf, wgs, wgr, wob, wds, wdb, gl, gb, zs2, zr2, ab, fs, fr, ob, hct, wab,
        send, recv, load, known,
    ) = refs
    (
        tok_ref, lens_ref, mem_ref, ngain_ref, wq_ref, wk_ref, wv_ref, wg_ref, wa_ref, wb_ref,
        dlog_ref, dbias_ref, hgain_ref, wout_ref, mgain_ref, wgate_ref, wup_ref, wdown_ref,
    ) = own
    kv = lax.axis_index("kv")
    tp = lax.axis_index("tp")
    z = kv // Y
    y = kv % Y
    group = y * TP + tp

    def y_peer(k):
        return z * Y + (y + k) % Y

    def z_peer(j):
        away = 8 - (j + 1) // 2
        return (z + Z + away * (2 * (j % 2) - 1)) % Z

    def hops(d):
        return min(d[0], Y - d[0]) + min(d[1], X - d[1])

    apart = [(dy, dx, dc) for dy in range(Y) for dx in range(X) for dc in range(2)][1:]
    apart = sorted(apart, key=hops, reverse=True)

    def group_peer(d):
        to_y, to_tp = (y + d[0]) % Y, (tp // 2 + d[1]) % X * 2 + (tp + d[2]) % 2
        return to_y * TP + to_tp, (z * Y + to_y, to_tp)

    barrier = pltpu.get_barrier_semaphore()

    def z_near(k):
        return (((z + k + Z) % Z) * Y + y, tp)

    loads = [pltpu.make_async_copy(hbm[k], own[k], load.at[k]) for k in range(IN_NAMES)]
    first = (0, 3, 4, 5, 6, 7, 8, 9)
    for k in first:
        loads[k].start()
    for k in (4, -4, 3, -3, 2, -2, 1, -1):
        pl.semaphore_signal(barrier, inc=1, device_id=z_near(k), device_id_type=MESH)
    for d in apart:
        pl.semaphore_signal(barrier, inc=1, device_id=group_peer(d)[1], device_id_type=MESH)
    for k in range(IN_NAMES):
        if k not in first:
            loads[k].start()
    for k in first:
        loads[k].wait()

    def rcopy(src, dst, phase, where):
        return pltpu.make_async_remote_copy(
            src_ref=src, dst_ref=dst, send_sem=send.at[phase], recv_sem=recv.at[phase],
            device_id=where, device_id_type=MESH,
        )

    def arrived(ref, phase):
        rcopy(ref, ref, phase, (y_peer(1), tp)).wait_recv()

    def sent(ref, phase):
        rcopy(ref, ref, phase, (y_peer(1), tp)).wait_send()

    at = iota((2 * ROWS, ROWS), 0)
    row = iota((2 * ROWS, ROWS), 1)
    slot = (at >> 3) & 15
    toward = (z + Z + (8 - ((slot + 1) >> 1)) * (2 * (slot & 1) - 1)) & 15
    wanted = 16 * toward + 4 * (at >> 7) + (at & 3)
    turn = jnp.where(row == wanted, 1.0, 0.0).astype(BF16)
    xt = mmt(turn, tok_ref[...])
    xs = (xt * ngain_ref[...]).astype(BF16)
    wab[...] = jnp.zeros((128, 64), BF16)
    wab[64:80, :] = wa_ref[...]
    wab[80:96, :] = wb_ref[...]
    squares = jnp.sum(xt * xt, axis=1, keepdims=True)
    high = squares.astype(BF16).astype(F32)
    low = squares - high
    eye = jnp.where(iota((64, 128), 0) == iota((64, 128), 1), 1.0, 0.0).astype(BF16)
    lane = iota((2 * ROWS, 128), 1)
    extra = mmt(xs, wab[...]) + mm(xt.astype(BF16), eye)
    extra = jnp.where(lane == 96, high, jnp.where(lane == 97, low, extra))
    second = (iota((2 * ROWS, 256), 0) & 4) == 4
    left = jnp.where(second, mm(xs, wv_ref[...]), mm(xs, wq_ref[...]))
    part[:, :, :, 0:256] = left.reshape(Y, Z, 8, 256).astype(BF16)
    right = jnp.where(second, mm(xs, wg_ref[...]), mm(xs, wk_ref[...]))
    part[:, :, :, 256:512] = right.reshape(Y, Z, 8, 256).astype(BF16)
    part[:, :, :, 512:640] = extra.reshape(Y, Z, 8, 128).astype(BF16)

    for k in range(IN_NAMES):
        if k not in first:
            loads[k].wait()
    for k in range(Y):
        wgs[k, :, 0:FFY] = wgate_ref[:, FFY * k : FFY * (k + 1)]
        wgs[k, :, FFY:FP] = jnp.zeros((64, FP - FFY), BF16)
        wgs[k, :, FP : FP + FFY] = wup_ref[:, FFY * k : FFY * (k + 1)]
        wgs[k, :, FP + FFY : W2] = jnp.zeros((64, FP - FFY), BF16)
        wds[k, :, 0:FFY] = wdown_ref[:, FFY * k : FFY * (k + 1)]
        wds[k, :, FFY:FP] = jnp.zeros((64, FP - FFY), BF16)
    gl[...] = jnp.zeros((8, 128), F32) + jnp.concatenate([mgain_ref[...], mgain_ref[...]], axis=1)

    pl.semaphore_wait(barrier, 8 + Y * TP - 1)

    for k in (4, -4):
        pl.semaphore_signal(known, inc=1, device_id=z_near(k), device_id_type=MESH)
    for c in range(PARTS):
        some = pl.ds(SLOTS * c, SLOTS)
        for k in range(1, Y):
            peer = y_peer(k)
            rcopy(part.at[peer % Y, some], yrecv.at[y, some], S_Y + c, (peer, tp)).start()
    for k in range(1, Y):
        peer = y_peer(k)
        rcopy(wout_ref, wob.at[y], S_WO, (peer, tp)).start()
        rcopy(wgs.at[peer % Y], wgr.at[y], S_WG, (peer, tp)).start()
        rcopy(wds.at[peer % Y], wdb.at[y], S_WD, (peer, tp)).start()
        rcopy(gl, gb.at[y], S_GN, (peer, tp)).start()

    yrecv[y] = part[y]
    wob[y] = wout_ref[...]
    wgr[y] = wgs[y]
    wdb[y] = wds[y]
    gb[y] = gl[...]

    def send_z1(j, c):
        to = z_peer(j)
        rcopy(zs1.at[j], zr1.at[z], S_Z, (to * Y + y, tp)).start()
        return c

    pl.semaphore_wait(known, 2)
    for c in range(PARTS):
        low, high_slot = SLOTS * c, SLOTS * (c + 1)
        arrived(yrecv.at[0:3, low:high_slot], S_Y + c)
        total = yrecv[0, low:high_slot].astype(F32)
        for k in range(1, Y):
            total = total + yrecv[k, low:high_slot].astype(F32)
        zs1[low:high_slot] = total.astype(BF16)
        lax.fori_loop(low, min(high_slot, Z - 1), send_z1, 0, unroll=True)
    zr1[z] = zs1[Z - 1]

    seq = iota((SEQS, ROWS), 0)
    lens8 = jnp.concatenate([lens_ref[...], lens_ref[...]], axis=1).astype(F32) + jnp.zeros((8, 128), F32)
    lens = lens8.T[0:SEQS, 0:1].astype(I32) + jnp.zeros((SEQS, ROWS), I32)
    place = iota((PLACES, ROWS), 0)

    def chooser(seq_of, slot):
        mine = jnp.sum(jnp.where(seq == seq_of, lens, 0), axis=0, keepdims=True)
        before = jnp.sum(jnp.where(seq < seq_of, lens, 0), axis=0, keepdims=True)
        slot = slot[0:1]
        index = before + slot
        chunk = (index * 9363) >> 16
        goes = jnp.where(slot < mine, index + chunk, -1)
        return jnp.where(place == goes, 1.0, 0.0).astype(BF16)

    col = iota((SEQS, ROWS), 1)
    pick = chooser(4 * ((col >> 2) & 15) + (col >> 6), col & 3)
    give = chooser(col >> 2, col & 3)

    arrived(zr1.at[0 : Z - 1], S_Z)

    mine = jnp.sum(zr1[...].astype(F32), axis=0)
    lane8 = iota((8, 128), 1)
    ext = mine[:, 512:640]

    def lane_of(values, where):
        return jnp.sum(jnp.where(lane8 == where, values, 0.0), axis=1, keepdims=True)

    rstd = lax.rsqrt((lane_of(ext, 96) + lane_of(ext, 97)) / D + EPS)
    main = (mine[:, 0:512] * rstd).astype(BF16).astype(F32)
    ext = ext * rstd
    length = jnp.sum(jnp.where(iota((1, SEQS), 1) == kv, lens_ref[...], 0), axis=1, keepdims=True)
    live = iota((8, 1), 0) < length
    rows = []
    for h in range(2):
        alpha = lane_of(ext, 64 + 2 * tp + h)
        beta = jax.nn.sigmoid(lane_of(ext, 80 + 2 * tp + h))
        shifted = alpha + dbias_ref[:, h : h + 1]
        soft = jnp.maximum(shifted, 0.0) + jnp.log1p(jnp.exp(-jnp.abs(shifted)))
        rate = jnp.exp(jnp.zeros((8, 1), F32) + dlog_ref[:, h : h + 1])
        decay = jnp.exp(jnp.where(live, -rate * soft, 0.0))
        beta = jnp.where(live, beta, 0.0)
        q8 = main[:, 128 * h : 128 * h + 128]
        k8 = main[:, 256 + 128 * h : 384 + 128 * h]
        q8 = q8 * lax.rsqrt(jnp.sum(q8 * q8, axis=1, keepdims=True) + EPS) * DK**-0.5
        k8 = k8 * lax.rsqrt(jnp.sum(k8 * k8, axis=1, keepdims=True) + EPS)
        qt, kt = q8.T, k8.T
        memory = mem_ref[0, h]
        for t in range(NEW):
            kcol = kt[:, t : t + 1]
            memory = memory * decay[t : t + 1]
            guess = jnp.sum(memory * kcol, axis=0, keepdims=True)
            fix = beta[t : t + 1] * (main[4 + t : 5 + t, 128 * h : 128 * h + 128] - guess)
            memory = memory + kcol * fix
            rows.append(jnp.sum(memory * qt[:, t : t + 1], axis=0, keepdims=True))
        nmem_ref[0, h] = memory
    attended = jnp.concatenate(rows, axis=0)
    attended = attended * lax.rsqrt(jnp.mean(attended * attended, axis=1, keepdims=True) + EPS)
    gates = jnp.concatenate([main[4:8, 256:384], main[4:8, 384:512]], axis=0)
    mixed = attended * hgain_ref[...] * (gates * jax.nn.sigmoid(gates))
    mrecv[z] = mixed.astype(BF16)

    def send_m(j, c):
        rcopy(mrecv.at[z], mrecv.at[z], S_M, (z_peer(j) * Y + y, tp)).start()
        return c

    lax.fori_loop(0, Z - 1, send_m, 0, unroll=True)
    arrived(wob.at[0:3], S_WO)
    wo = wob[...].reshape(256, 256)
    arrived(gb.at[0:3], S_GN)
    low_lane = iota((1, 128), 1) < 64
    gain = jnp.concatenate(
        [jnp.where(low_lane, gb[0, 0:1], gb[1, 0:1]), jnp.where(low_lane, gb[2, 0:1], gb[3, 0:1])], axis=1
    )
    low_half = iota((8, 128), 0) < 4

    def slot_of(where):
        away = (where - z + Z) % Z
        return (1 - away // 8) * (15 - 2 * away) + (away // 8) * (2 * away - 16)

    def kept(k):
        return jnp.where(
            low_half,
            yrecv[k, slot_of(2 * tp), :, 512:640].astype(F32),
            yrecv[k, slot_of(2 * tp + 1), :, 512:640].astype(F32),
        )

    residual = jnp.concatenate(
        [
            jnp.where(low_lane, kept(0), pltpu.roll(kept(1), 64, 1)),
            jnp.where(low_lane, kept(2), pltpu.roll(kept(3), 64, 1)),
        ],
        axis=1,
    )
    arrived(mrecv.at[0 : Z - 1], S_M)

    heads = mrecv[...].astype(F32).reshape(8 * Z, 128).astype(BF16)
    first_head = (iota((8 * Z, 256), 0) & 4) == 0
    terms = jnp.where(first_head, mmt(heads, wo[:, 0:128]), mmt(heads, wo[:, 128:256]))
    terms = terms.reshape(TP, 2, 8, 256)
    even, odd = terms[:, 0], terms[:, 1]
    even = even + jnp.concatenate([even[:, 4:8], even[:, 0:4]], axis=1)
    odd = odd + jnp.concatenate([odd[:, 4:8], odd[:, 0:4]], axis=1)
    cs[...] = jnp.where((iota((TP, 8, 256), 1) & 4) == 0, even, odd).astype(BF16)

    for d in apart:
        if d[0] == 0:
            other, where = group_peer(d)
            rcopy(cs.at[where[1]], cr.at[tp], S_C, where).start()
    cr[tp] = cs[tp]
    arrived(cr.at[0 : TP - 1], S_C)
    hbuf[group] = (residual + jnp.sum(cr[...].astype(F32), axis=0)).astype(BF16)

    for d in apart:
        other, where = group_peer(d)
        rcopy(hbuf.at[group], hbuf.at[group], S_H, where).start()
    arrived(wgr.at[0:3], S_WG)
    arrived(hbuf.at[0 : Y * TP - 1], S_H)

    hidden = mm(pick, hbuf[...].astype(F32).reshape(ROWS, 256).astype(BF16))
    hscaled = (hidden * gain).astype(BF16)
    products = mm(hscaled, wgr[...].reshape(256, W2))
    squares2 = jnp.sum(hidden * hidden, axis=1, keepdims=True)
    high2 = squares2.astype(BF16).astype(F32)
    low2 = squares2 - high2
    lane2 = iota((PLACES, W2), 1)
    products = jnp.where(lane2 == FFY, high2, jnp.where(lane2 == FFY + 1, low2, products))
    zs2[...] = products.reshape(Z, 8, W2).astype(BF16)

    def send_g(j, c):
        to = z_peer(j)
        rcopy(zs2.at[to], zr2.at[z], S_G, (to * Y + y, tp)).start()
        return c

    lax.fori_loop(0, Z - 1, send_g, 0, unroll=True)
    zr2[z] = zs2[z]
    hct[...] = hidden.T
    arrived(wdb.at[0:3], S_WD)
    arrived(zr2.at[0 : Z - 1], S_G)
    summed = jnp.sum(zr2[...].astype(F32), axis=0)
    lane3 = iota((8, FP), 1)
    gate, up = summed[:, 0:FP], summed[:, FP:W2]
    total2 = jnp.sum(jnp.where((lane3 == FFY) | (lane3 == FFY + 1), gate, 0.0), axis=1, keepdims=True)
    rstd2 = lax.rsqrt(total2 / D + EPS)
    gate = jnp.where(lane3 < FFY, gate, 0.0) * rstd2
    ab[z] = (gate * jax.nn.sigmoid(gate) * (up * rstd2)).astype(BF16)

    def send_a(j, c):
        rcopy(ab.at[z], ab.at[z], S_A, (z_peer(j) * Y + y, tp)).start()
        return c

    lax.fori_loop(0, Z - 1, send_a, 0, unroll=True)
    arrived(ab.at[0 : Z - 1], S_A)

    active = ab[...].astype(F32).reshape(PLACES, FP).astype(BF16)
    fs[...] = mmt(wdb[...].reshape(256, FP), active).reshape(Y * TP, 8, 128).astype(BF16)

    for d in apart:
        other, where = group_peer(d)
        rcopy(fs.at[other], fr.at[group], S_F, where).start()
    fr[group] = fs[group]
    arrived(fr.at[0 : Y * TP - 1], S_F)
    ended = jnp.sum(fr[...].astype(F32), axis=0) + hct[pl.ds(pl.multiple_of(8 * group, 8), 8), :]
    ob[tp] = ended.astype(BF16)

    for d in apart:
        if d[0] == 0:
            other, where = group_peer(d)
            rcopy(ob.at[tp], ob.at[tp], S_O, where).start()
    arrived(ob.at[0 : TP - 1], S_O)
    final = ob[...].astype(F32).reshape(64, PLACES).astype(BF16)
    out_ref[...] = mm(final, give).astype(BF16)

    for ref, phase in (
        (zr1.at[0 : Z - 1], S_Z), (mrecv.at[0 : Z - 1], S_M), (cr.at[0 : TP - 1], S_C),
        (hbuf.at[0 : Y * TP - 1], S_H), (zr2.at[0 : Z - 1], S_G), (ab.at[0 : Z - 1], S_A),
        (fr.at[0 : Y * TP - 1], S_F), (ob.at[0 : TP - 1], S_O), (wob.at[0:3], S_WO), (wgr.at[0:3], S_WG),
        (wdb.at[0:3], S_WD), (gb.at[0:3], S_GN),
    ):
        sent(ref, phase)
    for c in range(PARTS):
        sent(yrecv.at[0:3, 0:SLOTS], S_Y + c)


def deliver(result_ref, memory_ref, out_ref, new_ref):
    out_ref[...] = result_ref[...]
    new_ref[...] = memory_ref[...]


def per_device(
    tokens, lengths, memory, norm_gain, w_query, w_key, w_value, w_outgate, w_alpha, w_beta, decay_log, decay_bias,
    head_gain, w_output, mlp_gain, w_gate, w_up, w_down,
):
    inputs = (
        tokens.T, lengths[None], memory, norm_gain[None], w_query, w_key, w_value, w_outgate, w_alpha.T, w_beta.T,
        decay_log[None], decay_bias[None], head_gain[None], w_output.T, mlp_gain[None], w_gate, w_up, w_down.T,
    )
    outputs = (jax.ShapeDtypeStruct((64, ROWS), BF16), jax.ShapeDtypeStruct(memory.shape, F32))
    shapes = [((Y, Z, 8, W1), BF16)] * 2 + [((Z, 8, W1), BF16)] * 2 + [
        ((Z, 8, 128), BF16),
        ((TP, 8, 256), BF16),
        ((TP, 8, 256), BF16),
        ((Y * TP, 8, 256), BF16),
        ((Y, 64, W2), BF16),
        ((Y, 64, W2), BF16),
        ((Y, 64, 256), BF16),
        ((Y, 64, FP), BF16),
        ((Y, 64, FP), BF16),
        ((8, 128), F32),
        ((Y, 8, 128), F32),
        ((Z, 8, W2), BF16),
        ((Z, 8, W2), BF16),
        ((Z, 8, FP), BF16),
        ((Y * TP, 8, 128), BF16),
        ((Y * TP, 8, 128), BF16),
        ((TP, 8, 128), BF16),
        ((256, 128), F32),
        ((128, 64), BF16),
    ]
    result, new_memory = pl.pallas_call(
        kernel,
        out_shape=tuple(pltpu.VMEM(a.shape, a.dtype) for a in outputs),
        in_specs=[pl.BlockSpec(memory_space=pl.ANY)] * IN_NAMES,
        out_specs=tuple([pl.BlockSpec(memory_space=pltpu.VMEM)] * 2),
        scratch_shapes=[pltpu.VMEM(a.shape, a.dtype) for a in inputs]
        + [pltpu.VMEM(*shape) for shape in shapes]
        + [
            pltpu.SemaphoreType.DMA((PH,)),
            pltpu.SemaphoreType.DMA((PH,)),
            pltpu.SemaphoreType.DMA((IN_NAMES,)),
            pltpu.SemaphoreType.REGULAR,
        ],
        compiler_params=pltpu.CompilerParams(collective_id=0, has_side_effects=True),
    )(*inputs)
    vmem = pl.BlockSpec(memory_space=pltpu.VMEM)
    result, new_memory = pl.pallas_call(deliver, out_shape=outputs, in_specs=[vmem, vmem])(
        pltpu.with_memory_space_constraint(result, pltpu.VMEM),
        pltpu.with_memory_space_constraint(new_memory, pltpu.VMEM),
    )
    return (result.T, new_memory)


def solution(mesh):
    kv, tp = "kv", "tp"
    placed = (
        P(None, kv), P(), P(kv, tp, None, None), P(kv), P(kv, tp), P(kv, tp), P(kv, tp), P(kv, tp), P(kv, None),
        P(kv, None), P(tp), P(tp), P(), P(tp, kv), P(kv), P(kv, tp), P(kv, tp), P(tp, kv),
    )
    return jax.shard_map(
        per_device,
        mesh=mesh,
        in_specs=placed,
        out_specs=(P(None, kv), P(kv, tp, None, None)),
        check_vma=False,
    )
```

```python
import jax
import jax.numpy as jnp
from jax import lax
from jax.experimental import pallas as pl
from jax.experimental.pallas import tpu as pltpu
from jax.sharding import PartitionSpec as P

MESH = pl.DeviceIdType.MESH
F32, BF16, I32 = jnp.float32, jnp.bfloat16, jnp.int32
D, DK, NEW, SEQS = 4096, 128, 4, 64
Z, Y, X, TP = 16, 4, 4, 8
ROWS = SEQS * NEW
PLACES = 8 * Z
EPS = 1e-06
W1 = 640
FFZ = 176
FHALF = 192
FP = 2 * FHALF
PH = 17
S_Z, S_M, S_C, S_H, S_G, S_A, S_F, S_O, S_WO, S_WG, S_WD, S_GN, S_WZ, S_Y = range(PH - 3)
PARTS = 4
SLOTS = Z // PARTS


def iota(shape, dim):
    return lax.broadcasted_iota(I32, shape, dim)


def mm(a, b):
    return jnp.dot(a, b, preferred_element_type=F32)


IN_NAMES = 18


def mmt(a, b):
    return lax.dot_general(a, b, (((1,), (1,)), ((), ())), preferred_element_type=F32)


def kernel(*refs):
    hbm, (out_ref, nmem_ref) = refs[:IN_NAMES], refs[IN_NAMES : IN_NAMES + 2]
    refs = refs[IN_NAMES + 2 :]
    own, refs = refs[:IN_NAMES], refs[IN_NAMES:]
    (
        part, yrecv, zs1, zr1, mrecv, cs, cr, hbuf, wgs, wst, wgr, wob, wds, wdb, gl, gb, zs2, zr2, ab, fs, fr, ob, hct, wab,
        send, recv, load, known,
    ) = refs
    (
        tok_ref, lens_ref, mem_ref, ngain_ref, wq_ref, wk_ref, wv_ref, wg_ref, wa_ref, wb_ref,
        dlog_ref, dbias_ref, hgain_ref, wout_ref, mgain_ref, wgate_ref, wup_ref, wdown_ref,
    ) = own
    kv = lax.axis_index("kv")
    tp = lax.axis_index("tp")
    z = kv // Y
    y = kv % Y
    group = y * TP + tp
    bit = z % 2
    twin = z + 1 - 2 * bit

    def y_peer(k):
        return z * Y + (y + k) % Y

    def z_peer(j):
        away = 8 - (j + 1) // 2
        return (z + Z + away * (2 * (j % 2) - 1)) % Z

    def hops(d):
        return min(d[0], Y - d[0]) + min(d[1], X - d[1])

    apart = [(dy, dx, dc) for dy in range(Y) for dx in range(X) for dc in range(2)][1:]
    apart = sorted(apart, key=hops, reverse=True)

    def group_peer(d):
        to_y, to_tp = (y + d[0]) % Y, (tp // 2 + d[1]) % X * 2 + (tp + d[2]) % 2
        return to_y * TP + to_tp, (z * Y + to_y, to_tp)

    barrier = pltpu.get_barrier_semaphore()

    def z_near(k):
        return (((z + k + Z) % Z) * Y + y, tp)

    loads = [pltpu.make_async_copy(hbm[k], own[k], load.at[k]) for k in range(IN_NAMES)]
    first = (0, 3, 4, 5, 6, 7, 8, 9)
    for k in first:
        loads[k].start()
    for k in (4, -4, 3, -3, 2, -2, 1, -1):
        pl.semaphore_signal(barrier, inc=1, device_id=z_near(k), device_id_type=MESH)
    for d in apart:
        pl.semaphore_signal(barrier, inc=1, device_id=group_peer(d)[1], device_id_type=MESH)
    for k in range(IN_NAMES):
        if k not in first:
            loads[k].start()
    for k in first:
        loads[k].wait()

    def rcopy(src, dst, phase, where):
        return pltpu.make_async_remote_copy(
            src_ref=src, dst_ref=dst, send_sem=send.at[phase], recv_sem=recv.at[phase],
            device_id=where, device_id_type=MESH,
        )

    def arrived(ref, phase):
        rcopy(ref, ref, phase, (y_peer(1), tp)).wait_recv()

    def sent(ref, phase):
        rcopy(ref, ref, phase, (y_peer(1), tp)).wait_send()

    at = iota((2 * ROWS, ROWS), 0)
    row = iota((2 * ROWS, ROWS), 1)
    slot = (at >> 3) & 15
    toward = (z + Z + (8 - ((slot + 1) >> 1)) * (2 * (slot & 1) - 1)) & 15
    wanted = 16 * toward + 4 * (at >> 7) + (at & 3)
    turn = jnp.where(row == wanted, 1.0, 0.0).astype(BF16)
    xt = mmt(turn, tok_ref[...])
    xs = (xt * ngain_ref[...]).astype(BF16)
    wab[...] = jnp.zeros((128, 64), BF16)
    wab[64:80, :] = wa_ref[...]
    wab[80:96, :] = wb_ref[...]
    squares = jnp.sum(xt * xt, axis=1, keepdims=True)
    high = squares.astype(BF16).astype(F32)
    low = squares - high
    eye = jnp.where(iota((64, 128), 0) == iota((64, 128), 1), 1.0, 0.0).astype(BF16)
    lane = iota((2 * ROWS, 128), 1)
    extra = mmt(xs, wab[...]) + mm(xt.astype(BF16), eye)
    extra = jnp.where(lane == 96, high, jnp.where(lane == 97, low, extra))
    second = (iota((2 * ROWS, 256), 0) & 4) == 4
    left = jnp.where(second, mm(xs, wv_ref[...]), mm(xs, wq_ref[...]))
    part[:, :, :, 0:256] = left.reshape(Y, Z, 8, 256).astype(BF16)
    right = jnp.where(second, mm(xs, wg_ref[...]), mm(xs, wk_ref[...]))
    part[:, :, :, 256:512] = right.reshape(Y, Z, 8, 256).astype(BF16)
    part[:, :, :, 512:640] = extra.reshape(Y, Z, 8, 128).astype(BF16)

    for k in range(IN_NAMES):
        if k not in first:
            loads[k].wait()
    for k in range(Y):
        for n in range(2):
            cut, low = slice(FFZ * (2 * k + n), FFZ * (2 * k + n + 1)), FHALF * n
            wgs[n, k, :, 0:FFZ] = wgate_ref[:, cut]
            wgs[n, k, :, FFZ:FHALF] = jnp.zeros((64, FHALF - FFZ), BF16)
            wgs[n, k, :, FHALF : FHALF + FFZ] = wup_ref[:, cut]
            wgs[n, k, :, FHALF + FFZ : FP] = jnp.zeros((64, FHALF - FFZ), BF16)
            wds[k, :, low : low + FFZ] = wdown_ref[:, cut]
            wds[k, :, low + FFZ : low + FHALF] = jnp.zeros((64, FHALF - FFZ), BF16)
    gl[...] = jnp.zeros((8, 128), F32) + jnp.concatenate([mgain_ref[...], mgain_ref[...]], axis=1)

    pl.semaphore_wait(barrier, 8 + Y * TP - 1)

    for k in (4, -4):
        pl.semaphore_signal(known, inc=1, device_id=z_near(k), device_id_type=MESH)
    for c in range(PARTS):
        some = pl.ds(SLOTS * c, SLOTS)
        for k in range(1, Y):
            peer = y_peer(k)
            rcopy(part.at[peer % Y, some], yrecv.at[y, some], S_Y + c, (peer, tp)).start()
    rcopy(wgs.at[1 - bit], wst.at[bit], S_WZ, (twin * Y + y, tp)).start()
    for k in range(1, Y):
        peer = y_peer(k)
        rcopy(wout_ref, wob.at[y], S_WO, (peer, tp)).start()
        rcopy(wds.at[peer % Y], wdb.at[y], S_WD, (peer, tp)).start()
        rcopy(gl, gb.at[bit * Y + y], S_GN, (peer, tp)).start()

    yrecv[y] = part[y]
    wob[y] = wout_ref[...]
    wst[bit] = wgs[bit]
    wdb[y] = wds[y]
    gb[bit * Y + y] = gl[...]

    def send_z1(j, c):
        to = z_peer(j)
        rcopy(zs1.at[j], zr1.at[z], S_Z, (to * Y + y, tp)).start()
        return c

    pl.semaphore_wait(known, 2)
    for c in range(PARTS):
        low, high_slot = SLOTS * c, SLOTS * (c + 1)
        arrived(yrecv.at[0:3, low:high_slot], S_Y + c)
        total = yrecv[0, low:high_slot].astype(F32)
        for k in range(1, Y):
            total = total + yrecv[k, low:high_slot].astype(F32)
        zs1[low:high_slot] = total.astype(BF16)
        lax.fori_loop(low, min(high_slot, Z - 1), send_z1, 0, unroll=True)
    zr1[z] = zs1[Z - 1]
    arrived(wst.at[0], S_WZ)
    for k in range(Y):
        rcopy(gl, gb.at[bit * Y + y], S_GN, (twin * Y + (y + k) % Y, tp)).start()
    for k in range(1, Y):
        peer = y_peer(k)
        for n in range(2):
            rcopy(wst.at[n, peer % Y], wgr.at[n, y], S_WG, (peer, tp)).start()
    wgr[:, y] = wst[:, y]

    seq = iota((SEQS, ROWS), 0)
    lens8 = jnp.concatenate([lens_ref[...], lens_ref[...]], axis=1).astype(F32) + jnp.zeros((8, 128), F32)
    lens = lens8.T[0:SEQS, 0:1].astype(I32) + jnp.zeros((SEQS, ROWS), I32)
    place = iota((PLACES, ROWS), 0)

    def chooser(seq_of, slot):
        mine = jnp.sum(jnp.where(seq == seq_of, lens, 0), axis=0, keepdims=True)
        before = jnp.sum(jnp.where(seq < seq_of, lens, 0), axis=0, keepdims=True)
        slot = slot[0:1]
        index = before + slot
        chunk = (index * 9363) >> 16
        goes = jnp.where(slot < mine, index + chunk, -1)
        return jnp.where(place == goes, 1.0, 0.0).astype(BF16)

    col = iota((SEQS, ROWS), 1)
    pick = chooser(4 * ((col >> 2) & 15) + (col >> 6), col & 3)
    give = chooser(col >> 2, col & 3)

    arrived(zr1.at[0 : Z - 1], S_Z)

    mine = jnp.sum(zr1[...].astype(F32), axis=0)
    lane8 = iota((8, 128), 1)
    ext = mine[:, 512:640]

    def lane_of(values, where):
        return jnp.sum(jnp.where(lane8 == where, values, 0.0), axis=1, keepdims=True)

    rstd = lax.rsqrt((lane_of(ext, 96) + lane_of(ext, 97)) / D + EPS)
    main = (mine[:, 0:512] * rstd).astype(BF16).astype(F32)
    ext = ext * rstd
    length = jnp.sum(jnp.where(iota((1, SEQS), 1) == kv, lens_ref[...], 0), axis=1, keepdims=True)
    live = iota((8, 1), 0) < length
    rows = []
    for h in range(2):
        alpha = lane_of(ext, 64 + 2 * tp + h)
        beta = jax.nn.sigmoid(lane_of(ext, 80 + 2 * tp + h))
        shifted = alpha + dbias_ref[:, h : h + 1]
        soft = jnp.maximum(shifted, 0.0) + jnp.log1p(jnp.exp(-jnp.abs(shifted)))
        rate = jnp.exp(jnp.zeros((8, 1), F32) + dlog_ref[:, h : h + 1])
        decay = jnp.exp(jnp.where(live, -rate * soft, 0.0))
        beta = jnp.where(live, beta, 0.0)
        q8 = main[:, 128 * h : 128 * h + 128]
        k8 = main[:, 256 + 128 * h : 384 + 128 * h]
        q8 = q8 * lax.rsqrt(jnp.sum(q8 * q8, axis=1, keepdims=True) + EPS) * DK**-0.5
        k8 = k8 * lax.rsqrt(jnp.sum(k8 * k8, axis=1, keepdims=True) + EPS)
        qt, kt = q8.T, k8.T
        memory = mem_ref[0, h]
        for t in range(NEW):
            kcol = kt[:, t : t + 1]
            memory = memory * decay[t : t + 1]
            guess = jnp.sum(memory * kcol, axis=0, keepdims=True)
            fix = beta[t : t + 1] * (main[4 + t : 5 + t, 128 * h : 128 * h + 128] - guess)
            memory = memory + kcol * fix
            rows.append(jnp.sum(memory * qt[:, t : t + 1], axis=0, keepdims=True))
        nmem_ref[0, h] = memory
    attended = jnp.concatenate(rows, axis=0)
    attended = attended * lax.rsqrt(jnp.mean(attended * attended, axis=1, keepdims=True) + EPS)
    gates = jnp.concatenate([main[4:8, 256:384], main[4:8, 384:512]], axis=0)
    mixed = attended * hgain_ref[...] * (gates * jax.nn.sigmoid(gates))
    mrecv[z] = mixed.astype(BF16)

    def send_m(j, c):
        rcopy(mrecv.at[z], mrecv.at[z], S_M, (z_peer(j) * Y + y, tp)).start()
        return c

    lax.fori_loop(0, Z - 1, send_m, 0, unroll=True)
    arrived(wob.at[0:3], S_WO)
    wo = wob[...].reshape(256, 256)
    arrived(gb.at[0 : 2 * Y - 1], S_GN)
    low_lane = iota((1, 128), 1) < 64

    def gain_of(n):
        row = [gb[n * Y + k, 0:1] for k in range(Y)]
        return jnp.concatenate([jnp.where(low_lane, row[0], row[1]), jnp.where(low_lane, row[2], row[3])], axis=1)

    low_half = iota((8, 128), 0) < 4

    def slot_of(where):
        away = (where - z + Z) % Z
        return (1 - away // 8) * (15 - 2 * away) + (away // 8) * (2 * away - 16)

    def kept(k):
        return jnp.where(
            low_half,
            yrecv[k, slot_of(2 * tp), :, 512:640].astype(F32),
            yrecv[k, slot_of(2 * tp + 1), :, 512:640].astype(F32),
        )

    residual = jnp.concatenate(
        [
            jnp.where(low_lane, kept(0), pltpu.roll(kept(1), 64, 1)),
            jnp.where(low_lane, kept(2), pltpu.roll(kept(3), 64, 1)),
        ],
        axis=1,
    )
    arrived(mrecv.at[0 : Z - 1], S_M)

    heads = mrecv[...].astype(F32).reshape(8 * Z, 128).astype(BF16)
    first_head = (iota((8 * Z, 256), 0) & 4) == 0
    terms = jnp.where(first_head, mmt(heads, wo[:, 0:128]), mmt(heads, wo[:, 128:256]))
    terms = terms.reshape(TP, 2, 8, 256)
    even, odd = terms[:, 0], terms[:, 1]
    even = even + jnp.concatenate([even[:, 4:8], even[:, 0:4]], axis=1)
    odd = odd + jnp.concatenate([odd[:, 4:8], odd[:, 0:4]], axis=1)
    cs[...] = jnp.where((iota((TP, 8, 256), 1) & 4) == 0, even, odd).astype(BF16)

    for d in apart:
        if d[0] == 0:
            other, where = group_peer(d)
            rcopy(cs.at[where[1]], cr.at[tp], S_C, where).start()
    cr[tp] = cs[tp]
    arrived(cr.at[0 : TP - 1], S_C)
    place_h = bit * Y * TP + group
    hbuf[place_h] = (residual + jnp.sum(cr[...].astype(F32), axis=0)).astype(BF16)
    for d in apart + [(0, 0, 0)]:
        other, where = group_peer(d)
        rcopy(hbuf.at[place_h], hbuf.at[place_h], S_H, (where[0] + (twin - z) * Y, where[1])).start()
    for d in apart:
        other, where = group_peer(d)
        rcopy(hbuf.at[place_h], hbuf.at[place_h], S_H, where).start()
    arrived(wgr.at[:, 0:3], S_WG)
    gains = gain_of(bit), gain_of(1 - bit)
    arrived(hbuf.at[0 : 2 * Y * TP - 1], S_H)

    def chosen(n):
        return mm(pick, hbuf[pl.ds(n * Y * TP, Y * TP)].astype(F32).reshape(ROWS, 256).astype(BF16))

    hidden, beside = chosen(bit), chosen(1 - bit)
    products = mm((hidden * gains[0]).astype(BF16), wgr[bit].reshape(256, FP))
    products = products + mm((beside * gains[1]).astype(BF16), wgr[1 - bit].reshape(256, FP))
    squares2 = jnp.sum(hidden * hidden, axis=1, keepdims=True)
    high2 = squares2.astype(BF16).astype(F32)
    low2 = squares2 - high2
    lane2 = iota((PLACES, FP), 1)
    products = jnp.where(lane2 == FFZ, high2, jnp.where(lane2 == FFZ + 1, low2, products))
    zs2[...] = products.reshape(Z, 8, FP).astype(BF16)

    def send_g(j, c):
        to = z_peer(j)
        rcopy(zs2.at[to], zr2.at[z], S_G, (to * Y + y, tp)).start()
        return c

    lax.fori_loop(0, Z - 1, send_g, 0, unroll=True)
    zr2[z] = zs2[z]
    hct[...] = hidden.T
    arrived(wdb.at[0:3], S_WD)
    arrived(zr2.at[0 : Z - 1], S_G)
    summed = jnp.sum(zr2[...].astype(F32).reshape(Z // 2, 2, 8, FP), axis=0)
    lane3 = iota((8, FP), 1)
    both = summed[0] + summed[1]
    total2 = jnp.sum(jnp.where((lane3 == FFZ) | (lane3 == FFZ + 1), both, 0.0), axis=1, keepdims=True)
    rstd2 = lax.rsqrt(total2 / D + EPS)

    def activated(n):
        gate = jnp.where(lane3 < FFZ, summed[n], 0.0) * rstd2
        up = pltpu.roll(summed[n], FHALF, 1) * rstd2
        return gate * jax.nn.sigmoid(gate) * up

    ab[z] = (activated(0) + pltpu.roll(activated(1), FHALF, 1)).astype(BF16)

    def send_a(j, c):
        rcopy(ab.at[z], ab.at[z], S_A, (z_peer(j) * Y + y, tp)).start()
        return c

    lax.fori_loop(0, Z - 1, send_a, 0, unroll=True)
    arrived(ab.at[0 : Z - 1], S_A)

    active = ab[...].astype(F32).reshape(PLACES, FP).astype(BF16)
    fs[...] = mmt(wdb[...].reshape(256, FP), active).reshape(2 * Y, 32, 128).astype(BF16)
    x, core = tp // 2, tp % 2
    for d in apart:
        if d[1] == 0:
            to_y, to_core = (y + d[0]) % Y, (core + d[2]) % 2
            rcopy(fs.at[to_y * 2 + to_core], fr.at[y * 2 + core], S_F, (z * Y + to_y, x * 2 + to_core)).start()
    fr[y * 2 + core] = fs[y * 2 + core]
    arrived(fr.at[0 : 2 * Y - 1], S_F)
    ob[tp] = jnp.sum(fr[...].astype(F32), axis=0).astype(BF16)
    for d in apart:
        if d[0] == 0:
            other, where = group_peer(d)
            rcopy(ob.at[tp], ob.at[tp], S_O, where).start()
    arrived(ob.at[0 : TP - 1], S_O)
    fed = jnp.sum(ob[...].astype(F32).reshape(X, 64, 128), axis=0)
    final = (fed + hct[pl.ds(pl.multiple_of(64 * y, 64), 64), :]).astype(BF16)
    out_ref[...] = mm(final, give).astype(BF16)

    for ref, phase in (
        (zr1.at[0 : Z - 1], S_Z), (mrecv.at[0 : Z - 1], S_M), (cr.at[0 : TP - 1], S_C),
        (hbuf.at[0 : 2 * Y * TP - 1], S_H), (zr2.at[0 : Z - 1], S_G), (ab.at[0 : Z - 1], S_A),
        (fr.at[0 : 2 * Y - 1], S_F), (ob.at[0 : TP - 1], S_O), (wob.at[0:3], S_WO), (wgr.at[:, 0:3], S_WG), (wst.at[0], S_WZ),
        (wdb.at[0:3], S_WD), (gb.at[0 : 2 * Y - 1], S_GN),
    ):
        sent(ref, phase)
    for c in range(PARTS):
        sent(yrecv.at[0:3, 0:SLOTS], S_Y + c)


def deliver(result_ref, memory_ref, out_ref, new_ref):
    out_ref[...] = result_ref[...]
    new_ref[...] = memory_ref[...]


def per_device(
    tokens, lengths, memory, norm_gain, w_query, w_key, w_value, w_outgate, w_alpha, w_beta, decay_log, decay_bias,
    head_gain, w_output, mlp_gain, w_gate, w_up, w_down,
):
    inputs = (
        tokens.T, lengths[None], memory, norm_gain[None], w_query, w_key, w_value, w_outgate, w_alpha.T, w_beta.T,
        decay_log[None], decay_bias[None], head_gain[None], w_output.T, mlp_gain[None], w_gate, w_up, w_down.T,
    )
    outputs = (jax.ShapeDtypeStruct((64, ROWS), BF16), jax.ShapeDtypeStruct(memory.shape, F32))
    shapes = [((Y, Z, 8, W1), BF16)] * 2 + [((Z, 8, W1), BF16)] * 2 + [
        ((Z, 8, 128), BF16),
        ((TP, 8, 256), BF16),
        ((TP, 8, 256), BF16),
        ((2 * Y * TP, 8, 256), BF16),
        ((2, Y, 64, FP), BF16),
        ((2, Y, 64, FP), BF16),
        ((2, Y, 64, FP), BF16),
        ((Y, 64, 256), BF16),
        ((Y, 64, FP), BF16),
        ((Y, 64, FP), BF16),
        ((8, 128), F32),
        ((2 * Y, 8, 128), F32),
        ((Z, 8, FP), BF16),
        ((Z, 8, FP), BF16),
        ((Z, 8, FP), BF16),
        ((2 * Y, 32, 128), BF16),
        ((2 * Y, 32, 128), BF16),
        ((TP, 32, 128), BF16),
        ((256, 128), F32),
        ((128, 64), BF16),
    ]
    result, new_memory = pl.pallas_call(
        kernel,
        out_shape=tuple(pltpu.VMEM(a.shape, a.dtype) for a in outputs),
        in_specs=[pl.BlockSpec(memory_space=pl.ANY)] * IN_NAMES,
        out_specs=tuple([pl.BlockSpec(memory_space=pltpu.VMEM)] * 2),
        scratch_shapes=[pltpu.VMEM(a.shape, a.dtype) for a in inputs]
        + [pltpu.VMEM(*shape) for shape in shapes]
        + [
            pltpu.SemaphoreType.DMA((PH,)),
            pltpu.SemaphoreType.DMA((PH,)),
            pltpu.SemaphoreType.DMA((IN_NAMES,)),
            pltpu.SemaphoreType.REGULAR,
        ],
        compiler_params=pltpu.CompilerParams(collective_id=0, has_side_effects=True),
    )(*inputs)
    vmem = pl.BlockSpec(memory_space=pltpu.VMEM)
    result, new_memory = pl.pallas_call(deliver, out_shape=outputs, in_specs=[vmem, vmem])(
        pltpu.with_memory_space_constraint(result, pltpu.VMEM),
        pltpu.with_memory_space_constraint(new_memory, pltpu.VMEM),
    )
    return (result.T, new_memory)


def solution(mesh):
    kv, tp = "kv", "tp"
    placed = (
        P(None, kv), P(), P(kv, tp, None, None), P(kv), P(kv, tp), P(kv, tp), P(kv, tp), P(kv, tp), P(kv, None),
        P(kv, None), P(tp), P(tp), P(), P(tp, kv), P(kv), P(kv, tp), P(kv, tp), P(tp, kv),
    )
    return jax.shard_map(
        per_device,
        mesh=mesh,
        in_specs=placed,
        out_specs=(P(None, kv), P(kv, tp, None, None)),
        check_vma=False,
    )
```

```python
import jax
import jax.numpy as jnp
from jax import lax
from jax.experimental import pallas as pl
from jax.experimental.pallas import tpu as pltpu
from jax.sharding import PartitionSpec as P

MESH = pl.DeviceIdType.MESH
F32, BF16, I32 = jnp.float32, jnp.bfloat16, jnp.int32
D, DK, NEW, SEQS = 4096, 128, 4, 64
Z, Y, X, TP = 16, 4, 4, 8
ROWS = SEQS * NEW
PLACES = 8 * Z
EPS = 1e-06
W1 = 512
FFZ = 176
FHALF = 192
FP = 2 * FHALF
S_Z, S_M, S_C, S_H, S_G, S_A, S_F, S_O, S_WO, S_WG, S_WD, S_GN, S_WZ, S_TK, S_EY, S_EZ, S_Y = range(17)
PARTS = 8
PH = 17 + PARTS
SLOTS = Z // PARTS


def iota(shape, dim):
    return lax.broadcasted_iota(I32, shape, dim)


def mm(a, b):
    return jnp.dot(a, b, preferred_element_type=F32)


IN_NAMES = 18


def mmt(a, b):
    return lax.dot_general(a, b, (((1,), (1,)), ((), ())), preferred_element_type=F32)


def kernel(*refs):
    hbm, (out_ref, nmem_ref) = refs[:IN_NAMES], refs[IN_NAMES : IN_NAMES + 2]
    refs = refs[IN_NAMES + 2 :]
    own, refs = refs[:IN_NAMES], refs[IN_NAMES:]
    (
        part, yrecv, zs1, zr1, eys, eyr, ezs, ezr, tks, tkr, mrecv, cs, cr, hbuf, wgs, wst, wgr, wob, wds, wdb, gl, gb, zs2, zr2, ab, fs, fr, ob, hct,
        send, recv, load, known,
    ) = refs
    (
        tok_ref, lens_ref, mem_ref, ngain_ref, wq_ref, wk_ref, wv_ref, wg_ref, wa_ref, wb_ref,
        dlog_ref, dbias_ref, hgain_ref, wout_ref, mgain_ref, wgate_ref, wup_ref, wdown_ref,
    ) = own
    kv = lax.axis_index("kv")
    tp = lax.axis_index("tp")
    z = kv // Y
    y = kv % Y
    group = y * TP + tp
    bit = z % 2
    twin = z + 1 - 2 * bit

    def y_peer(k):
        return z * Y + (y + k) % Y

    def z_peer(j):
        away = 8 - (j + 1) // 2
        return (z + Z + away * (2 * (j % 2) - 1)) % Z

    def hops(d):
        return min(d[0], Y - d[0]) + min(d[1], X - d[1])

    apart = [(dy, dx, dc) for dy in range(Y) for dx in range(X) for dc in range(2)][1:]
    apart = sorted(apart, key=hops, reverse=True)

    def group_peer(d):
        to_y, to_tp = (y + d[0]) % Y, (tp // 2 + d[1]) % X * 2 + (tp + d[2]) % 2
        return to_y * TP + to_tp, (z * Y + to_y, to_tp)

    barrier = pltpu.get_barrier_semaphore()

    def z_near(k):
        return (((z + k + Z) % Z) * Y + y, tp)

    loads = [pltpu.make_async_copy(hbm[k], own[k], load.at[k]) for k in range(IN_NAMES)]
    first = (0, 3, 4, 5, 6, 7, 8, 9)
    for k in first:
        loads[k].start()
    for k in (4, -4, 3, -3, 2, -2, 1, -1):
        pl.semaphore_signal(barrier, inc=1, device_id=z_near(k), device_id_type=MESH)
    for d in apart:
        pl.semaphore_signal(barrier, inc=1, device_id=group_peer(d)[1], device_id_type=MESH)
    for k in range(IN_NAMES):
        if k not in first:
            loads[k].start()
    for k in first:
        loads[k].wait()

    def rcopy(src, dst, phase, where):
        return pltpu.make_async_remote_copy(
            src_ref=src, dst_ref=dst, send_sem=send.at[phase], recv_sem=recv.at[phase],
            device_id=where, device_id_type=MESH,
        )

    def arrived(ref, phase):
        rcopy(ref, ref, phase, (y_peer(1), tp)).wait_recv()

    def sent(ref, phase):
        rcopy(ref, ref, phase, (y_peer(1), tp)).wait_send()

    at = iota((2 * ROWS, ROWS), 0)
    row = iota((2 * ROWS, ROWS), 1)
    slot = (at >> 3) & 15
    toward = (z + Z + (8 - ((slot + 1) >> 1)) * (2 * (slot & 1) - 1)) & 15
    wanted = 16 * toward + 4 * (at >> 7) + (at & 3)
    turn = jnp.where(row == wanted, 1.0, 0.0).astype(BF16)
    xt = mmt(turn, tok_ref[...])
    xs = (xt * ngain_ref[...]).astype(BF16)
    kind, source = iota((128, 32), 0) & 7, iota((128, 32), 1)
    both_w = jnp.concatenate([wa_ref[...], wb_ref[...]], axis=0)
    from_where = jnp.where(kind < 2, 2 * tp + kind, 14 + 2 * tp + kind)
    chosen_w = jnp.where((source == from_where) & (kind < 4), 1.0, 0.0).astype(BF16)
    wab = mm(chosen_w, both_w).astype(BF16)
    squares = jnp.sum(xt * xt, axis=1, keepdims=True)
    eye = jnp.where(iota((64, 128), 0) == iota((64, 128), 1), 1.0, 0.0).astype(BF16)
    lane = iota((2 * ROWS, 128), 1)
    extra = jnp.where((lane & 7) == 4, squares, mmt(xs, wab))
    extra = jnp.where((lane >> 3) == (iota((2 * ROWS, 128), 0) & 7), extra, 0.0)
    eys[...] = jnp.sum(extra.reshape(Y, Z, 8, 128), axis=2)
    tks[...] = mm(xt.astype(BF16), eye).reshape(Y, Z, 8, 128).astype(BF16)
    second = (iota((2 * ROWS, 256), 0) & 4) == 4
    left = jnp.where(second, mm(xs, wv_ref[...]), mm(xs, wq_ref[...]))
    part[:, :, :, 0:256] = left.reshape(Y, Z, 8, 256).astype(BF16)
    right = jnp.where(second, mm(xs, wg_ref[...]), mm(xs, wk_ref[...]))
    part[:, :, :, 256:512] = right.reshape(Y, Z, 8, 256).astype(BF16)

    for k in range(IN_NAMES):
        if k not in first:
            loads[k].wait()
    for k in range(Y):
        for n in range(2):
            cut, low = slice(FFZ * (2 * k + n), FFZ * (2 * k + n + 1)), FHALF * n
            wgs[n, k, :, 0:FFZ] = wgate_ref[:, cut]
            wgs[n, k, :, FFZ:FHALF] = jnp.zeros((64, FHALF - FFZ), BF16)
            wgs[n, k, :, FHALF : FHALF + FFZ] = wup_ref[:, cut]
            wgs[n, k, :, FHALF + FFZ : FP] = jnp.zeros((64, FHALF - FFZ), BF16)
            wds[k, :, low : low + FFZ] = wdown_ref[:, cut]
            wds[k, :, low + FFZ : low + FHALF] = jnp.zeros((64, FHALF - FFZ), BF16)
    gl[...] = jnp.zeros((8, 128), F32) + jnp.concatenate([mgain_ref[...], mgain_ref[...]], axis=1)

    pl.semaphore_wait(barrier, 8 + Y * TP - 1)

    for k in (4, -4):
        pl.semaphore_signal(known, inc=1, device_id=z_near(k), device_id_type=MESH)
    for k in range(1, Y):
        peer = y_peer(k)
        rcopy(eys.at[peer % Y], eyr.at[y], S_EY, (peer, tp)).start()
    for c in range(PARTS):
        some = pl.ds(SLOTS * c, SLOTS)
        for k in range(1, Y):
            peer = y_peer(k)
            rcopy(part.at[peer % Y, some], yrecv.at[y, some], S_Y + c, (peer, tp)).start()
    rcopy(wgs.at[1 - bit], wst.at[bit], S_WZ, (twin * Y + y, tp)).start()
    for k in range(1, Y):
        peer = y_peer(k)
        rcopy(wout_ref, wob.at[y], S_WO, (peer, tp)).start()
        rcopy(tks.at[peer % Y], tkr.at[y], S_TK, (peer, tp)).start()
        rcopy(wds.at[peer % Y], wdb.at[y], S_WD, (peer, tp)).start()
        rcopy(gl, gb.at[bit * Y + y], S_GN, (peer, tp)).start()

    yrecv[y] = part[y]
    eyr[y] = eys[y]
    tkr[y] = tks[y]
    wob[y] = wout_ref[...]
    wst[bit] = wgs[bit]
    wdb[y] = wds[y]
    gb[bit * Y + y] = gl[...]

    def send_z1(j, c):
        to = z_peer(j)
        rcopy(zs1.at[j], zr1.at[z], S_Z, (to * Y + y, tp)).start()
        return c

    def send_e(j, c):
        to = z_peer(j)
        rcopy(ezs.at[j], ezr.at[z], S_EZ, (to * Y + y, tp)).start()
        return c

    arrived(eyr.at[0:3], S_EY)
    lines = eyr[0]
    for k in range(1, Y):
        lines = lines + eyr[k]
    ezs[...] = lines.reshape(Z, 1, 128)
    ezr[z] = ezs[Z - 1]
    pl.semaphore_wait(known, 2)
    lax.fori_loop(0, Z - 1, send_e, 0, unroll=True)
    for c in range(PARTS):
        low, high_slot = SLOTS * c, SLOTS * (c + 1)
        arrived(yrecv.at[0:3, low:high_slot], S_Y + c)
        total = yrecv[0, low:high_slot].astype(F32)
        for k in range(1, Y):
            total = total + yrecv[k, low:high_slot].astype(F32)
        zs1[low:high_slot] = total.astype(BF16)
        lax.fori_loop(low, min(high_slot, Z - 1), send_z1, 0, unroll=True)
    zr1[z] = zs1[Z - 1]
    arrived(wst.at[0], S_WZ)
    for k in range(Y):
        rcopy(gl, gb.at[bit * Y + y], S_GN, (twin * Y + (y + k) % Y, tp)).start()
    for k in range(1, Y):
        peer = y_peer(k)
        for n in range(2):
            rcopy(wst.at[n, peer % Y], wgr.at[n, y], S_WG, (peer, tp)).start()
    wgr[:, y] = wst[:, y]

    seq = iota((SEQS, ROWS), 0)
    lens8 = jnp.concatenate([lens_ref[...], lens_ref[...]], axis=1).astype(F32) + jnp.zeros((8, 128), F32)
    lens = lens8.T[0:SEQS, 0:1].astype(I32) + jnp.zeros((SEQS, ROWS), I32)
    place = iota((PLACES, ROWS), 0)

    def chooser(seq_of, slot):
        mine = jnp.sum(jnp.where(seq == seq_of, lens, 0), axis=0, keepdims=True)
        before = jnp.sum(jnp.where(seq < seq_of, lens, 0), axis=0, keepdims=True)
        slot = slot[0:1]
        index = before + slot
        chunk = (index * 9363) >> 16
        goes = jnp.where(slot < mine, index + chunk, -1)
        return jnp.where(place == goes, 1.0, 0.0).astype(BF16)

    col = iota((SEQS, ROWS), 1)
    pick = chooser(4 * ((col >> 2) & 15) + (col >> 6), col & 3)
    give = chooser(col >> 2, col & 3)

    arrived(zr1.at[0 : Z - 1], S_Z)

    mine = jnp.sum(zr1[...].astype(F32), axis=0)
    arrived(ezr.at[0 : Z - 1], S_EZ)
    ext = jnp.sum(ezr[...], axis=0)
    lane8 = iota((8, 128), 1)
    slot8 = 8 * (iota((8, 128), 0) & 3)

    def lane_of(values, where):
        return jnp.sum(jnp.where(lane8 == slot8 + where, values, 0.0), axis=1, keepdims=True)

    rstd = lax.rsqrt(lane_of(ext, 4) / D + EPS)
    main = (mine * rstd).astype(BF16).astype(F32)
    length = jnp.sum(jnp.where(iota((1, SEQS), 1) == kv, lens_ref[...], 0), axis=1, keepdims=True)
    live = iota((8, 1), 0) < length
    rows = []
    for h in range(2):
        alpha = lane_of(ext, h) * rstd
        beta = jax.nn.sigmoid(lane_of(ext, 2 + h) * rstd)
        shifted = alpha + dbias_ref[:, h : h + 1]
        soft = jnp.maximum(shifted, 0.0) + jnp.log1p(jnp.exp(-jnp.abs(shifted)))
        rate = jnp.exp(jnp.zeros((8, 1), F32) + dlog_ref[:, h : h + 1])
        decay = jnp.exp(jnp.where(live, -rate * soft, 0.0))
        beta = jnp.where(live, beta, 0.0)
        q8 = main[:, 128 * h : 128 * h + 128]
        k8 = main[:, 256 + 128 * h : 384 + 128 * h]
        q8 = q8 * lax.rsqrt(jnp.sum(q8 * q8, axis=1, keepdims=True) + EPS) * DK**-0.5
        k8 = k8 * lax.rsqrt(jnp.sum(k8 * k8, axis=1, keepdims=True) + EPS)
        qt, kt = q8.T, k8.T
        memory = mem_ref[0, h]
        for t in range(NEW):
            kcol = kt[:, t : t + 1]
            memory = memory * decay[t : t + 1]
            guess = jnp.sum(memory * kcol, axis=0, keepdims=True)
            fix = beta[t : t + 1] * (main[4 + t : 5 + t, 128 * h : 128 * h + 128] - guess)
            memory = memory + kcol * fix
            rows.append(jnp.sum(memory * qt[:, t : t + 1], axis=0, keepdims=True))
        nmem_ref[0, h] = memory
    attended = jnp.concatenate(rows, axis=0)
    attended = attended * lax.rsqrt(jnp.mean(attended * attended, axis=1, keepdims=True) + EPS)
    gates = jnp.concatenate([main[4:8, 256:384], main[4:8, 384:512]], axis=0)
    mixed = attended * hgain_ref[...] * (gates * jax.nn.sigmoid(gates))
    mrecv[z] = mixed.astype(BF16)

    def send_m(j, c):
        rcopy(mrecv.at[z], mrecv.at[z], S_M, (z_peer(j) * Y + y, tp)).start()
        return c

    lax.fori_loop(0, Z - 1, send_m, 0, unroll=True)
    arrived(wob.at[0:3], S_WO)
    wo = wob[...].reshape(256, 256)
    arrived(gb.at[0 : 2 * Y - 1], S_GN)
    low_lane = iota((1, 128), 1) < 64

    def gain_of(n):
        row = [gb[n * Y + k, 0:1] for k in range(Y)]
        return jnp.concatenate([jnp.where(low_lane, row[0], row[1]), jnp.where(low_lane, row[2], row[3])], axis=1)

    low_half = iota((8, 128), 0) < 4

    def slot_of(where):
        away = (where - z + Z) % Z
        return (1 - away // 8) * (15 - 2 * away) + (away // 8) * (2 * away - 16)

    arrived(tkr.at[0:3], S_TK)

    def kept(k):
        return jnp.where(
            low_half,
            tkr[k, slot_of(2 * tp)].astype(F32),
            tkr[k, slot_of(2 * tp + 1)].astype(F32),
        )

    residual = jnp.concatenate(
        [
            jnp.where(low_lane, kept(0), pltpu.roll(kept(1), 64, 1)),
            jnp.where(low_lane, kept(2), pltpu.roll(kept(3), 64, 1)),
        ],
        axis=1,
    )
    arrived(mrecv.at[0 : Z - 1], S_M)

    heads = mrecv[...].astype(F32).reshape(8 * Z, 128).astype(BF16)
    first_head = (iota((8 * Z, 256), 0) & 4) == 0
    terms = jnp.where(first_head, mmt(heads, wo[:, 0:128]), mmt(heads, wo[:, 128:256]))
    terms = terms.reshape(TP, 2, 8, 256)
    even, odd = terms[:, 0], terms[:, 1]
    even = even + jnp.concatenate([even[:, 4:8], even[:, 0:4]], axis=1)
    odd = odd + jnp.concatenate([odd[:, 4:8], odd[:, 0:4]], axis=1)
    cs[...] = jnp.where((iota((TP, 8, 256), 1) & 4) == 0, even, odd).astype(BF16)

    for d in apart:
        if d[0] == 0:
            other, where = group_peer(d)
            rcopy(cs.at[where[1]], cr.at[tp], S_C, where).start()
    cr[tp] = cs[tp]
    arrived(cr.at[0 : TP - 1], S_C)
    place_h = bit * Y * TP + group
    hbuf[place_h] = (residual + jnp.sum(cr[...].astype(F32), axis=0)).astype(BF16)
    for d in apart + [(0, 0, 0)]:
        other, where = group_peer(d)
        rcopy(hbuf.at[place_h], hbuf.at[place_h], S_H, (where[0] + (twin - z) * Y, where[1])).start()
    for d in apart:
        other, where = group_peer(d)
        rcopy(hbuf.at[place_h], hbuf.at[place_h], S_H, where).start()
    arrived(wgr.at[:, 0:3], S_WG)
    gains = gain_of(bit), gain_of(1 - bit)
    arrived(hbuf.at[0 : 2 * Y * TP - 1], S_H)

    def chosen(n):
        return mm(pick, hbuf[pl.ds(n * Y * TP, Y * TP)].astype(F32).reshape(ROWS, 256).astype(BF16))

    hidden, beside = chosen(bit), chosen(1 - bit)
    products = mm((hidden * gains[0]).astype(BF16), wgr[bit].reshape(256, FP))
    products = products + mm((beside * gains[1]).astype(BF16), wgr[1 - bit].reshape(256, FP))
    squares2 = jnp.sum(hidden * hidden, axis=1, keepdims=True)
    high2 = squares2.astype(BF16).astype(F32)
    low2 = squares2 - high2
    lane2 = iota((PLACES, FP), 1)
    products = jnp.where(lane2 == FFZ, high2, jnp.where(lane2 == FFZ + 1, low2, products))
    zs2[...] = products.reshape(Z, 8, FP).astype(BF16)

    def send_g(j, c):
        to = z_peer(j)
        rcopy(zs2.at[to], zr2.at[z], S_G, (to * Y + y, tp)).start()
        return c

    lax.fori_loop(0, Z - 1, send_g, 0, unroll=True)
    zr2[z] = zs2[z]
    hct[...] = hidden.T
    arrived(wdb.at[0:3], S_WD)
    arrived(zr2.at[0 : Z - 1], S_G)
    summed = jnp.sum(zr2[...].astype(F32).reshape(Z // 2, 2, 8, FP), axis=0)
    lane3 = iota((8, FP), 1)
    both = summed[0] + summed[1]
    total2 = jnp.sum(jnp.where((lane3 == FFZ) | (lane3 == FFZ + 1), both, 0.0), axis=1, keepdims=True)
    rstd2 = lax.rsqrt(total2 / D + EPS)

    def activated(n):
        gate = jnp.where(lane3 < FFZ, summed[n], 0.0) * rstd2
        up = pltpu.roll(summed[n], FHALF, 1) * rstd2
        return gate * jax.nn.sigmoid(gate) * up

    ab[z] = (activated(0) + pltpu.roll(activated(1), FHALF, 1)).astype(BF16)

    def send_a(j, c):
        rcopy(ab.at[z], ab.at[z], S_A, (z_peer(j) * Y + y, tp)).start()
        return c

    lax.fori_loop(0, Z - 1, send_a, 0, unroll=True)
    arrived(ab.at[0 : Z - 1], S_A)

    active = ab[...].astype(F32).reshape(PLACES, FP).astype(BF16)
    fs[...] = mmt(wdb[...].reshape(256, FP), active).reshape(2 * Y, 32, 128).astype(BF16)
    x, core = tp // 2, tp % 2
    for d in apart:
        if d[1] == 0:
            to_y, to_core = (y + d[0]) % Y, (core + d[2]) % 2
            rcopy(fs.at[to_y * 2 + to_core], fr.at[y * 2 + core], S_F, (z * Y + to_y, x * 2 + to_core)).start()
    fr[y * 2 + core] = fs[y * 2 + core]
    arrived(fr.at[0 : 2 * Y - 1], S_F)
    ob[tp] = jnp.sum(fr[...].astype(F32), axis=0).astype(BF16)
    for d in apart:
        if d[0] == 0:
            other, where = group_peer(d)
            rcopy(ob.at[tp], ob.at[tp], S_O, where).start()
    arrived(ob.at[0 : TP - 1], S_O)
    fed = jnp.sum(ob[...].astype(F32).reshape(X, 64, 128), axis=0)
    final = (fed + hct[pl.ds(pl.multiple_of(64 * y, 64), 64), :]).astype(BF16)
    out_ref[...] = mm(final, give).astype(BF16)

    for ref, phase in (
        (zr1.at[0 : Z - 1], S_Z), (tkr.at[0:3], S_TK), (eyr.at[0:3], S_EY), (ezr.at[0 : Z - 1], S_EZ), (mrecv.at[0 : Z - 1], S_M), (cr.at[0 : TP - 1], S_C),
        (hbuf.at[0 : 2 * Y * TP - 1], S_H), (zr2.at[0 : Z - 1], S_G), (ab.at[0 : Z - 1], S_A),
        (fr.at[0 : 2 * Y - 1], S_F), (ob.at[0 : TP - 1], S_O), (wob.at[0:3], S_WO), (wgr.at[:, 0:3], S_WG), (wst.at[0], S_WZ),
        (wdb.at[0:3], S_WD), (gb.at[0 : 2 * Y - 1], S_GN),
    ):
        sent(ref, phase)
    for c in range(PARTS):
        sent(yrecv.at[0:3, 0:SLOTS], S_Y + c)


def deliver(result_ref, memory_ref, out_ref, new_ref):
    out_ref[...] = result_ref[...]
    new_ref[...] = memory_ref[...]


def per_device(
    tokens, lengths, memory, norm_gain, w_query, w_key, w_value, w_outgate, w_alpha, w_beta, decay_log, decay_bias,
    head_gain, w_output, mlp_gain, w_gate, w_up, w_down,
):
    inputs = (
        tokens.T, lengths[None], memory, norm_gain[None], w_query, w_key, w_value, w_outgate, w_alpha.T, w_beta.T,
        decay_log[None], decay_bias[None], head_gain[None], w_output.T, mlp_gain[None], w_gate, w_up, w_down.T,
    )
    outputs = (jax.ShapeDtypeStruct((64, ROWS), BF16), jax.ShapeDtypeStruct(memory.shape, F32))
    shapes = [((Y, Z, 8, W1), BF16)] * 2 + [((Z, 8, W1), BF16)] * 2 + [
        ((Y, Z, 128), F32),
        ((Y, Z, 128), F32),
        ((Z, 1, 128), F32),
        ((Z, 1, 128), F32),
        ((Y, Z, 8, 128), BF16),
        ((Y, Z, 8, 128), BF16),
        ((Z, 8, 128), BF16),
        ((TP, 8, 256), BF16),
        ((TP, 8, 256), BF16),
        ((2 * Y * TP, 8, 256), BF16),
        ((2, Y, 64, FP), BF16),
        ((2, Y, 64, FP), BF16),
        ((2, Y, 64, FP), BF16),
        ((Y, 64, 256), BF16),
        ((Y, 64, FP), BF16),
        ((Y, 64, FP), BF16),
        ((8, 128), F32),
        ((2 * Y, 8, 128), F32),
        ((Z, 8, FP), BF16),
        ((Z, 8, FP), BF16),
        ((Z, 8, FP), BF16),
        ((2 * Y, 32, 128), BF16),
        ((2 * Y, 32, 128), BF16),
        ((TP, 32, 128), BF16),
        ((256, 128), F32),
    ]
    result, new_memory = pl.pallas_call(
        kernel,
        out_shape=tuple(pltpu.VMEM(a.shape, a.dtype) for a in outputs),
        in_specs=[pl.BlockSpec(memory_space=pl.ANY)] * IN_NAMES,
        out_specs=tuple([pl.BlockSpec(memory_space=pltpu.VMEM)] * 2),
        scratch_shapes=[pltpu.VMEM(a.shape, a.dtype) for a in inputs]
        + [pltpu.VMEM(*shape) for shape in shapes]
        + [
            pltpu.SemaphoreType.DMA((PH,)),
            pltpu.SemaphoreType.DMA((PH,)),
            pltpu.SemaphoreType.DMA((IN_NAMES,)),
            pltpu.SemaphoreType.REGULAR,
        ],
        compiler_params=pltpu.CompilerParams(collective_id=0, has_side_effects=True),
    )(*inputs)
    vmem = pl.BlockSpec(memory_space=pltpu.VMEM)
    result, new_memory = pl.pallas_call(deliver, out_shape=outputs, in_specs=[vmem, vmem])(
        pltpu.with_memory_space_constraint(result, pltpu.VMEM),
        pltpu.with_memory_space_constraint(new_memory, pltpu.VMEM),
    )
    return (result.T, new_memory)


def solution(mesh):
    kv, tp = "kv", "tp"
    placed = (
        P(None, kv), P(), P(kv, tp, None, None), P(kv), P(kv, tp), P(kv, tp), P(kv, tp), P(kv, tp), P(kv, None),
        P(kv, None), P(tp), P(tp), P(), P(tp, kv), P(kv), P(kv, tp), P(kv, tp), P(tp, kv),
    )
    return jax.shard_map(
        per_device,
        mesh=mesh,
        in_specs=placed,
        out_specs=(P(None, kv), P(kv, tp, None, None)),
        check_vma=False,
    )
```
